512 devices in a mesh: vp: 128 (over z, x, core), dp: 4 (over y).
Axes of the slice: x: 4, y: 4, z: 16, core: 2. Of those that a mesh axis runs over, the one named last changes fastest.
Arguments:
- stream: bfloat16 [1024, 2048], P(('dp', 'vp')), may hold values from -60 to 60
- hidden: bfloat16 [1024, 5632], P('dp', 'vp'), may hold values from -6 to 6
- w_down: bfloat16 [5632, 2048], P(None, 'vp'), may hold values from -0.078125 to 0.078125
- final_gain: float32 [2048], replicated, may hold values from 0.1 to 1.9
- vocab: bfloat16 [2048, 32768], P(None, 'vp'), may hold values from -2 to 200
- vocab_bias: float32 [32768], P('vp'), may hold values from -5 to 5
- targets: int32 [1024], P('dp'), may hold values from 0 to 32767
Outputs:
- losses: float32 [1024], P(('dp', 'vp'))
- grad_input: float32 [1024, 2048], P(('dp', 'vp'))
- grad_vocab: float32 [2048, 32768], P('dp', 'vp')
The draws below stay inside these ranges and needn't reach their ends.
All inputs are finite; a program needn't handle non-finite values.
Results may differ from the reference program's by a relative error of at most 0.02.
Values may be sent and summed in bfloat16 or wider, within the bound.
No kernel may reach another device: no remote copies, remote signals or barrier semaphores. Data moves between devices by JAX's collectives and lax.ppermute only.
A program may use at most 64 MiB of HBM per device.

```python
import math
import jax
import jax.numpy as jnp
import numpy as np
from jax import lax

D = 2048
FF = 5632
VOCAB = 32768
TOK_GROUP = 256
TOKENS = 1024
COLS_DEV = 256


def draw_stream(key, part):
    ramp = 3.0 ** (jnp.arange(D, dtype=jnp.float32) / (D - 1))
    base = jnp.clip(jax.random.normal(key, (TOKENS, D), jnp.float32), -6.0, 6.0)
    values = base * ramp
    return values.astype(jnp.bfloat16)


def draw_vocab(key, part):
    base = jnp.clip(jax.random.normal(key, (D, VOCAB), jnp.float32), -6.0, 6.0) * (2.5 / math.sqrt(D))
    return base.astype(jnp.bfloat16)


def draw_vocab_bias(key, part):
    shards = VOCAB // COLS_DEV
    shard = (jnp.arange(VOCAB, dtype=jnp.int32) // COLS_DEV).astype(jnp.float32)
    ramp = 2.0 * shard / max(shards - 1, 1) - 1.0
    noise = jnp.clip(jax.random.normal(key, (VOCAB,), jnp.float32), -4.0, 4.0)
    return 0.5 * noise + ramp


def with_ends(result, own_key, least, largest):
    place = [jax.random.randint(jax.random.fold_in(own_key, axis), (), 0, length) for axis, length in enumerate(result.shape)]
    widest = result.shape.index(max(result.shape))
    next_to = place[:widest] + [(place[widest] + 1) % result.shape[widest]] + place[widest + 1:]
    return result.at[tuple(place)].set(least).at[tuple(next_to)].set(largest)


def steps_of(key, shape, cuts, low, high):
    gain, own = 1.0, jax.random.fold_in(key, 6)
    for position, shards_of in cuts:
        draws = jnp.exp(jax.random.uniform(jax.random.fold_in(own, position), (shards_of,), jnp.float32, low / len(cuts), high / len(cuts)))
        gain = gain * jnp.repeat(draws, shape[position] // shards_of).reshape([-1 if axis == position else 1 for axis in range(len(shape))])
    return gain


def rank_table(amount, lean):
    portions = [(1 << 20) // math.isqrt(standing ** lean) + 1 for standing in range(1, amount + 1)]
    width = 1 + sum(portions) // (1 << 30)
    return np.cumsum(np.array([max(1, weight // width) for weight in portions]))


def ranked_ids(own_key, dims, count, lean):
    listing = rank_table(count, lean)
    pick = jax.random.randint(jax.random.fold_in(own_key, 1), dims, 0, int(listing[count - 1]))
    standing = jnp.searchsorted(jnp.asarray(listing, jnp.int32), pick, side="right")
    return jax.random.permutation(jax.random.fold_in(own_key, 2), count)[standing].astype(jnp.int32)


def centred(own_key, dims, deviation, reach, split=(), kind=jnp.bfloat16):
    result = deviation * jax.random.normal(own_key, dims, jnp.float32)
    if split:
        result = result * steps_of(own_key, dims, split, -0.22, 0.18)
    return jnp.clip(result, -reach, reach).astype(kind)


def setup_inputs(seed: int = 0) -> dict:
    key_list = jax.random.split(jax.random.key(seed), 8)
    return {
        "stream": draw_stream(jax.random.fold_in(key_list[7], 71), 0),
        "hidden": centred(key_list[1], (TOKENS, FF), 1.0, 6.0, ((0, 4), (1, 128))),
        "w_down": centred(key_list[2], (FF, D), FF ** -0.5, 0.078125, ((1, 128),)),
        "final_gain": jnp.clip(1.0 + 0.18 * jax.random.normal(key_list[3], (D,), jnp.float32), 0.1, 1.9),
        "vocab": draw_vocab(jax.random.fold_in(key_list[7], 71), 0),
        "vocab_bias": draw_vocab_bias(jax.random.fold_in(key_list[7], 71), 0),
        "targets": with_ends(ranked_ids(key_list[6], (TOKENS,), VOCAB, 2), jax.random.fold_in(key_list[6], 3), 0, VOCAB - 1).astype(jnp.int32),
    }


norm_eps = 1e-06
zloss_weight = 0.001

def reference(stream, hidden, w_down, final_gain, vocab, vocab_bias, targets):
    proj = jnp.dot(hidden, w_down, preferred_element_type=jnp.float32)
    normin = (stream.astype(jnp.float32) + proj).astype(jnp.bfloat16)
    values = normin.astype(jnp.float32)
    inv = lax.rsqrt(lax.optimization_barrier(jnp.mean(values * values, axis=1, keepdims=True)) + norm_eps)
    normed = (values * inv * final_gain).astype(jnp.bfloat16)
    groups = TOKENS // TOK_GROUP
    normed_blocks = normed.reshape(groups, TOK_GROUP, D)
    target_blocks = targets.reshape(groups, TOK_GROUP)

    def one_group(carry, inputs):
        rows, goal = inputs
        scores = jnp.dot(rows, vocab, preferred_element_type=jnp.float32) + vocab_bias
        top = lax.optimization_barrier(jnp.max(scores, axis=1))
        lse = top + jnp.log(lax.optimization_barrier(jnp.sum(jnp.exp(scores - top[:, None]), axis=1)))
        hit = lax.broadcasted_iota(jnp.int32, (TOK_GROUP, VOCAB), 1) == goal[:, None]
        target_score = lax.optimization_barrier(jnp.sum(jnp.where(hit, scores, 0.0), axis=1))
        losses = lse - target_score + zloss_weight * lse * lse
        probs = jnp.exp(scores - lse[:, None])
        dscore = (probs * (1.0 + 2.0 * zloss_weight * lse)[:, None] - jnp.where(hit, 1.0, 0.0)).astype(jnp.bfloat16)
        drows = jnp.dot(dscore, vocab.T, preferred_element_type=jnp.float32)
        carry = carry + jnp.dot(rows.T, dscore, preferred_element_type=jnp.float32)
        return (carry, (losses, drows))
    grad_vocab, (losses, drows) = lax.scan(one_group, jnp.zeros((D, VOCAB), jnp.float32), (normed_blocks, target_blocks))
    dnormed = drows.reshape(TOKENS, D)
    scaled = dnormed * final_gain
    grad_input = inv * (scaled - values * inv * inv * lax.optimization_barrier(jnp.mean(values * scaled, axis=1, keepdims=True)))
    return (losses.reshape(TOKENS), grad_input, grad_vocab)
```

```python
import jax
import jax.numpy as jnp
from jax import lax
from jax.sharding import Mesh
from jax.sharding import PartitionSpec as P

Z = "vp_0"
Q = ("vp_1", "vp_2")
VP = ("vp_0", "vp_1", "vp_2")
DP_VP = ("dp", "vp_0", "vp_1", "vp_2")

norm_eps = 1e-06
zloss_weight = 0.001
f32 = jnp.float32
bf16 = jnp.bfloat16


def exchange(blocks, axes):
    return lax.all_to_all(blocks, axes, split_axis=0, concat_axis=0, tiled=True)


def shared(block, axes, count):
    return exchange(jnp.broadcast_to(block[None], (count, *block.shape)), axes)


def dot(a, b, da, db):
    return lax.dot_general(a, b, (((da,), (db,)), ((), ())), preferred_element_type=f32)


def merged(stats):
    top = jnp.max(stats[:, 0], axis=0)
    lse = top + jnp.log(jnp.sum(jnp.exp(stats[:, 0] - top), axis=0))
    return jnp.stack([lse, jnp.sum(stats[:, 1], axis=0)])


def body(stream, hidden, w_down, final_gain, vocab, vocab_bias, targets):
    nz, nq = lax.axis_size(Z), lax.axis_size(Q)
    ny = lax.axis_size("dp")
    own, width = stream.shape
    group, units = hidden.shape
    cols = w_down.shape[1]
    ncols = vocab.shape[1]
    z, mine = lax.axis_index(Z), lax.axis_index(VP)
    feats = nz * cols
    span = nq * own
    part = stream.reshape(own, nz, nq, cols).transpose(2, 0, 1, 3).reshape(nq, own, feats)
    units_all = jnp.broadcast_to(hidden.T[None], (nq, units, group))
    first = exchange(jnp.concatenate([units_all, part], axis=1), Q)
    hid = first[:, :units].reshape(nq * units, group)
    rows = first[:, units:].reshape(span, feats)
    w_rows = exchange(w_down.T.reshape(cols, nz, nq * units).transpose(1, 0, 2), Z)
    w_rows = w_rows.reshape(feats, nq * units)
    place = lax.broadcasted_iota(jnp.int32, (span, group), 1) - z * span
    place = (place == lax.broadcasted_iota(jnp.int32, (span, group), 0)).astype(bf16)
    partial = dot(w_rows, hid, 1, 0) + dot(rows, place, 0, 0)
    arrived = exchange(partial.reshape(nz, cols, group), Z)
    normin = jnp.sum(arrived, axis=0).astype(bf16)
    by_z = shared(normin, Z, nz)
    by_q = shared(by_z, Q, nq)
    normin = by_q.transpose(1, 0, 2, 3).reshape(width, group)
    values = normin.astype(f32)
    inv = lax.rsqrt(jnp.mean(values * values, axis=0, keepdims=True) + norm_eps)
    normed = (values * inv * final_gain[:, None]).astype(bf16)

    scores = dot(vocab, normed, 0, 0) + vocab_bias[:, None]
    top = jnp.max(scores, axis=0)
    local = top + jnp.log(jnp.sum(jnp.exp(scores - top), axis=0))
    ids = lax.broadcasted_iota(jnp.int32, (ncols, group), 0) + mine * ncols
    hit = ids == targets[None, :]
    goal = jnp.sum(jnp.where(hit, scores, 0.0), axis=0)
    stats = merged(shared(jnp.stack([local, goal]), Q, nq))
    stats = merged(shared(stats, Z, nz))
    lse = stats[0]
    losses = lse - stats[1] + zloss_weight * lse * lse
    losses = lax.dynamic_slice_in_dim(losses, mine * own, own)
    dscore = (jnp.exp(scores - lse) * (1.0 + 2.0 * zloss_weight * lse) - jnp.where(hit, 1.0, 0.0)).astype(bf16)

    feat_group = width // ny
    normed_y = exchange(normed.reshape(ny, feat_group, group), "dp")
    dscore_y = shared(dscore, "dp", ny)
    grad_vocab = sum(dot(normed_y[g], dscore_y[g], 1, 1) for g in range(ny))

    line = lax.broadcasted_iota(jnp.int32, (group, group), 0)
    token = (line // own) % nz * span + line // (own * nz) * own + line % own
    order = (token == lax.broadcasted_iota(jnp.int32, (group, group), 1)).astype(bf16)
    dscore_rows = dot(order, dscore, 1, 1).astype(bf16)
    row_term = dot(dscore_rows, vocab, 1, 1).astype(bf16)
    row_q = exchange(row_term.reshape(nq, nz * own, width), Q)
    row_q = jnp.sum(row_q.astype(f32), axis=0).astype(bf16)
    row_z = exchange(row_q.reshape(nz, own, width), Z)
    dnormed = jnp.sum(row_z.astype(f32), axis=0)

    pick = lax.broadcasted_iota(jnp.int32, (own, group), 0) + mine * own
    pick = (pick == lax.broadcasted_iota(jnp.int32, (own, group), 1)).astype(bf16)
    values = dot(pick, normin, 1, 1)
    inv = lax.rsqrt(jnp.mean(values * values, axis=1, keepdims=True) + norm_eps)
    scaled = dnormed * final_gain
    grad_input = inv * (
        scaled - values * inv * inv * jnp.mean(values * scaled, axis=1, keepdims=True)
    )
    return (losses, grad_input, grad_vocab)


def solution(mesh):
    torus = Mesh(mesh.devices.reshape(16, 4, 2, mesh.shape["dp"]), ("vp_0", "vp_1", "vp_2", "dp"))
    return jax.shard_map(
        body,
        mesh=torus,
        in_specs=(P(DP_VP, None), P("dp", VP), P(None, VP), P(), P(None, VP), P(VP), P("dp")),
        out_specs=(P(DP_VP), P(DP_VP, None), P("dp", VP)),
        check_vma=False,
    )
```

```python
import jax
import jax.numpy as jnp
from jax import lax
from jax.sharding import Mesh
from jax.sharding import PartitionSpec as P

Z = "vp_0"
Q = ("vp_1", "vp_2")
VP = ("vp_0", "vp_1", "vp_2")
DP_VP = ("dp", "vp_0", "vp_1", "vp_2")

norm_eps = 1e-06
zloss_weight = 0.001
f32 = jnp.float32
bf16 = jnp.bfloat16


def exchange(blocks, axes):
    return lax.all_to_all(blocks, axes, split_axis=0, concat_axis=0, tiled=True)


def shared(block, axes, count):
    return exchange(jnp.broadcast_to(block[None], (count, *block.shape)), axes)


def partner(array, axes, step):
    return lax.ppermute(array, axes, [(k, k ^ step) for k in range(lax.axis_size(axes))])


def dot(a, b, da, db):
    return lax.dot_general(a, b, (((da,), (db,)), ((), ())), preferred_element_type=f32)


def merged(stats):
    top = jnp.max(stats[:, 0], axis=0)
    lse = top + jnp.log(jnp.sum(jnp.exp(stats[:, 0] - top), axis=0))
    return jnp.stack([lse, jnp.sum(stats[:, 1], axis=0)])


def body(stream, hidden, w_down, final_gain, vocab, vocab_bias, targets):
    nz, nq, ny = lax.axis_size(Z), lax.axis_size(Q), lax.axis_size("dp")
    own, width = stream.shape
    group, units = hidden.shape
    cols = w_down.shape[1]
    ncols = vocab.shape[1]
    z, q, y, mine = lax.axis_index(Z), lax.axis_index(Q), lax.axis_index("dp"), lax.axis_index(VP)
    span = nz * own
    feats = nq * cols
    rows = -(-(units + own) // 16) * 16

    line = lax.broadcasted_iota(jnp.int32, (group, group), 0)
    token = (line // own) % nz * (nq * own) + line // span * own + line % own
    order = token == lax.broadcasted_iota(jnp.int32, (group, group), 1)
    goals = jnp.sum(jnp.where(order, targets[None, :], 0), axis=1)

    mine_h = dot(hidden, order.astype(bf16), 0, 1).astype(bf16)
    part = stream.reshape(own, nz, feats).transpose(1, 0, 2)
    part = jnp.pad(part, ((0, 0), (0, rows - units - own), (0, group - feats)))
    first = jnp.concatenate([jnp.broadcast_to(mine_h[None], (nz, units, group)), part], axis=1)
    first = exchange(first, Z)

    blocks = w_down.T.reshape(cols, nz, nq, units).transpose(2, 0, 1, 3)
    blocks = jnp.pad(blocks, ((0, 0), (0, 0), (0, 0), (0, rows - units)))
    blocks = blocks.reshape(nq, cols, nz * rows)
    w_rows = jnp.zeros_like(blocks)
    for step in range(nq):
        block = lax.dynamic_slice_in_dim(blocks, q ^ step, 1)
        block = partner(block, Q, step) if step else block
        w_rows = lax.dynamic_update_slice_in_dim(w_rows, block, q ^ step, 0)

    partial = dot(first.reshape(nz * rows, group), w_rows.reshape(feats, nz * rows), 0, 1)
    proj = jnp.sum(exchange(partial.reshape(nq, span, feats), Q), axis=0)
    row_part = first[:, units : units + own, :feats].reshape(span, feats)
    normin = (row_part.astype(f32) + proj).astype(bf16)
    normin = shared(normin, Z, nz).transpose(1, 0, 2).reshape(span, width)
    values = normin.astype(f32)
    inv = lax.rsqrt(jnp.mean(values * values, axis=1, keepdims=True) + norm_eps)
    normed = (values * inv * final_gain).astype(bf16)
    normed = shared(normed, Q, nq).reshape(group, width)

    scores = dot(normed, vocab, 1, 0) + vocab_bias
    top = jnp.max(scores, axis=1)
    local = top + jnp.log(jnp.sum(jnp.exp(scores - top[:, None]), axis=1))
    ids = lax.broadcasted_iota(jnp.int32, (group, ncols), 1) + mine * ncols
    hit = ids == goals[:, None]
    goal = jnp.sum(jnp.where(hit, scores, 0.0), axis=1)
    stats = merged(shared(jnp.stack([local, goal]), Q, nq))
    stats = merged(shared(stats, Z, nz))
    lse = stats[0]
    losses = lse - stats[1] + zloss_weight * lse * lse
    losses = lax.dynamic_slice_in_dim(losses, q * span + z * own, own)
    scale = 1.0 + 2.0 * zloss_weight * lse
    dscore = jnp.exp(scores - lse[:, None]) * scale[:, None] - jnp.where(hit, 1.0, 0.0)
    dscore = dscore.astype(bf16)

    feat_group = width // ny
    grad_vocab = 0.0
    for step in range(ny):
        piece = lax.dynamic_slice_in_dim(normed, (y ^ step) * feat_group, feat_group, 1)
        other = dscore
        if step:
            piece, other = partner(piece, "dp", step), partner(dscore, "dp", step)
        grad_vocab = grad_vocab + dot(piece, other, 0, 0)

    row_term = dot(dscore, vocab, 1, 1).astype(bf16)
    row_q = exchange(row_term.reshape(nq, span, width), Q)
    row_q = jnp.sum(row_q.astype(f32), axis=0).astype(bf16)
    row_z = exchange(row_q.reshape(nz, own, width), Z)
    dnormed = jnp.sum(row_z.astype(f32), axis=0)

    values = lax.dynamic_slice_in_dim(values, z * own, own)
    inv = lax.dynamic_slice_in_dim(inv, z * own, own)
    scaled = dnormed * final_gain
    grad_input = inv * (
        scaled - values * inv * inv * jnp.mean(values * scaled, axis=1, keepdims=True)
    )
    return (losses, grad_input, grad_vocab)


def solution(mesh):
    torus = Mesh(mesh.devices.reshape(16, 4, 2, mesh.shape["dp"]), ("vp_0", "vp_1", "vp_2", "dp"))
    return jax.shard_map(
        body,
        mesh=torus,
        in_specs=(P(DP_VP, None), P("dp", VP), P(None, VP), P(), P(None, VP), P(VP), P("dp")),
        out_specs=(P(DP_VP), P(DP_VP, None), P("dp", VP)),
        check_vma=False,
    )
```

```python
import jax
import jax.numpy as jnp
import numpy as np
from jax import lax
from jax.sharding import Mesh
from jax.sharding import PartitionSpec as P

Z, X, C = "vp_0", "vp_1", "vp_2"
Q = ("vp_1", "vp_2")
VP = ("vp_0", "vp_1", "vp_2")
DP_VP = ("dp", "vp_0", "vp_1", "vp_2")

norm_eps = 1e-06
zloss_weight = 0.001
f32 = jnp.float32
bf16 = jnp.bfloat16


def exchange(blocks, axes):
    return lax.all_to_all(blocks, axes, split_axis=0, concat_axis=0, tiled=True)


def shared(block, axes, count):
    return exchange(jnp.broadcast_to(block[None], (count, *block.shape)), axes)


def partner(array, axes, step):
    return lax.ppermute(array, axes, [(k, k ^ step) for k in range(lax.axis_size(axes))])


def dot(a, b, da, db):
    return lax.dot_general(a, b, (((da,), (db,)), ((), ())), preferred_element_type=f32)


def merged(stats):
    top = jnp.max(stats[:, 0], axis=0)
    lse = top + jnp.log(jnp.sum(jnp.exp(stats[:, 0] - top), axis=0))
    return jnp.stack([lse, jnp.sum(stats[:, 1], axis=0)])


def halves(array, core):
    first = lax.dynamic_slice_in_dim(array, core * (array.shape[0] // 2), array.shape[0] // 2)
    other = (1 - core) * (array.shape[0] // 2)
    return first, lax.dynamic_slice_in_dim(array, other, array.shape[0] // 2)


def body(stream, hidden, w_down, final_gain, vocab, vocab_bias, targets):
    nz, nx, nc, ny = (lax.axis_size(a) for a in (Z, X, C, "dp"))
    z, x, c, y = (lax.axis_index(a) for a in (Z, X, C, "dp"))
    nq = nx * nc
    own, width = stream.shape
    group, units = hidden.shape
    cols = w_down.shape[1]
    ncols = vocab.shape[1]
    mine = (z * nx + x) * nc + c
    span = nz * own
    half = nx * span
    feats = nq * cols
    rows = -(-(units + own) // 16) * 16

    order = np.arange(group).reshape(nz, nq, own).transpose(1, 0, 2).reshape(-1)
    order = jnp.asarray(np.eye(group, dtype=np.float32)[order], bf16)
    mine_h = dot(hidden, order, 0, 1).astype(bf16)
    part = stream.reshape(own, nz, feats).transpose(1, 0, 2)
    part = jnp.pad(part, ((0, 0), (units, rows - units - own), (0, group - feats)))
    mine_h = jnp.pad(mine_h, ((0, rows - units), (0, 0)))
    first = exchange(mine_h[None] + part, Z)

    blocks = w_down.T.reshape(cols, nz, nq, units).transpose(2, 0, 1, 3)
    blocks = jnp.pad(blocks, ((0, 0), (0, 0), (0, 0), (0, rows - units)))
    blocks = blocks.reshape(nx, nc, cols, nz * rows).transpose(1, 0, 2, 3)
    kept, sent = halves(blocks, c)
    came = partner(sent, C, 1)
    pair = jnp.concatenate([jnp.where(c == 0, kept, came), jnp.where(c == 0, came, kept)], axis=0)
    pair = pair.transpose(1, 0, 2, 3)
    w_rows = jnp.zeros_like(pair)
    for step in range(nx):
        block = lax.dynamic_slice_in_dim(pair, x ^ step, 1)
        block = partner(block, X, step) if step else block
        w_rows = lax.dynamic_update_slice_in_dim(w_rows, block, x ^ step, 0)

    partial = dot(first.reshape(nz * rows, group), w_rows.reshape(feats, nz * rows), 0, 1)
    proj = jnp.sum(exchange(partial.reshape(nq, span, feats), Q), axis=0)
    row_part = first[:, units : units + own, :feats].reshape(span, feats)
    normin = (row_part.astype(f32) + proj).astype(bf16)
    normin = shared(normin, Z, nz).transpose(1, 0, 2).reshape(span, width)
    values = normin.astype(f32)
    inv = lax.rsqrt(jnp.mean(values * values, axis=1, keepdims=True) + norm_eps)
    normed = (values * inv * final_gain).astype(bf16)
    normed = shared(normed, X, nx).reshape(half, width)
    normed = (normed, partner(normed, C, 1))

    line = lax.broadcasted_iota(jnp.int32, (group, group), 0)
    token = (line // own) % nz * (nq * own) + (line // span) % nx * (nc * own) + line // half * own + line % own
    goals = jnp.where(token == lax.broadcasted_iota(jnp.int32, (group, group), 1), targets[None, :], 0)
    goals = halves(jnp.sum(goals, axis=1), c)
    ids = lax.broadcasted_iota(jnp.int32, (half, ncols), 1) + mine * ncols
    hit = [ids == g[:, None] for g in goals]
    scores = [dot(n, vocab, 1, 0) + vocab_bias for n in normed]
    stats = []
    for s, h in zip(scores, hit):
        top = jnp.max(s, axis=1)
        local = top + jnp.log(jnp.sum(jnp.exp(s - top[:, None]), axis=1))
        stats.append(jnp.stack([local, jnp.sum(jnp.where(h, s, 0.0), axis=1)]))
    stats = jnp.where(c == 0, jnp.concatenate(stats, axis=1), jnp.concatenate(stats[::-1], axis=1))
    stats = merged(shared(stats, Q, nq))
    stats = merged(shared(stats, Z, nz))
    lse, goal = stats
    losses = lse - goal + zloss_weight * lse * lse
    losses = lax.dynamic_slice_in_dim(losses, c * half + x * span + z * own, own)
    dscore = []
    for s, h, l in zip(scores, hit, halves(lse, c)):
        scale = 1.0 + 2.0 * zloss_weight * l
        d = jnp.exp(s - l[:, None]) * scale[:, None] - jnp.where(h, 1.0, 0.0)
        dscore.append(d.astype(bf16))

    sent = dot(dscore[1], vocab, 1, 1).astype(bf16)
    came = partner(sent, C, 1)
    row_term = (dot(dscore[0], vocab, 1, 1) + came.astype(f32)).astype(bf16)

    row_term, *dscore = lax.optimization_barrier((row_term, *dscore))
    feat_group = width // ny
    grad_vocab = 0.0
    for step in range(ny):
        at = (y ^ step) * feat_group
        pieces = [lax.dynamic_slice_in_dim(n, at, feat_group, 1) for n in normed]
        both = jnp.concatenate([jnp.concatenate([p, d], axis=1) for p, d in zip(pieces, dscore)])
        both = partner(both, "dp", step) if step else both
        grad_vocab = grad_vocab + dot(both[:, :feat_group], both[:, feat_group:], 0, 0)

    row_x = exchange(row_term.reshape(nx, span, width), X)
    row_x = jnp.sum(row_x.astype(f32), axis=0).astype(bf16)
    row_z = exchange(row_x.reshape(nz, own, width), Z)
    dnormed = jnp.sum(row_z.astype(f32), axis=0)

    values = lax.dynamic_slice_in_dim(values, z * own, own)
    inv = lax.dynamic_slice_in_dim(inv, z * own, own)
    scaled = dnormed * final_gain
    grad_input = inv * (
        scaled - values * inv * inv * jnp.mean(values * scaled, axis=1, keepdims=True)
    )
    return (losses, grad_input, grad_vocab)


def solution(mesh):
    torus = Mesh(mesh.devices.reshape(16, 4, 2, mesh.shape["dp"]), ("vp_0", "vp_1", "vp_2", "dp"))
    return jax.shard_map(
        body,
        mesh=torus,
        in_specs=(P(DP_VP, None), P("dp", VP), P(None, VP), P(), P(None, VP), P(VP), P("dp")),
        out_specs=(P(DP_VP), P(DP_VP, None), P("dp", VP)),
        check_vma=False,
    )
```

```python
import jax
import jax.numpy as jnp
import numpy as np
from jax import lax
from jax.sharding import Mesh
from jax.sharding import PartitionSpec as P

Z, X, C = "vp_0", "vp_1", "vp_2"
Q = ("vp_1", "vp_2")
VP = ("vp_0", "vp_1", "vp_2")
DP_VP = ("dp", "vp_0", "vp_1", "vp_2")

norm_eps = 1e-06
zloss_weight = 0.001
f32 = jnp.float32
bf16 = jnp.bfloat16


def exchange(blocks, axes):
    return lax.all_to_all(blocks, axes, split_axis=0, concat_axis=0, tiled=True)


def shared(block, axes, count):
    return exchange(jnp.broadcast_to(block[None], (count, *block.shape)), axes)


def partner(array, axes, step):
    return lax.ppermute(array, axes, [(k, k ^ step) for k in range(lax.axis_size(axes))])


def dot(a, b, da, db):
    return lax.dot_general(a, b, (((da,), (db,)), ((), ())), preferred_element_type=f32)


def merged(stats):
    top = jnp.max(stats[:, 0], axis=0)
    lse = top + jnp.log(jnp.sum(jnp.exp(stats[:, 0] - top), axis=0))
    return jnp.stack([lse, jnp.sum(stats[:, 1], axis=0)])


def halves(array, core):
    first = lax.dynamic_slice_in_dim(array, core * (array.shape[0] // 2), array.shape[0] // 2)
    other = (1 - core) * (array.shape[0] // 2)
    return first, lax.dynamic_slice_in_dim(array, other, array.shape[0] // 2)


def body(stream, hidden, w_down, final_gain, vocab, vocab_bias, targets):
    nz, nx, nc, ny = (lax.axis_size(a) for a in (Z, X, C, "dp"))
    z, x, c, y = (lax.axis_index(a) for a in (Z, X, C, "dp"))
    nq = nx * nc
    own, width = stream.shape
    group, units = hidden.shape
    cols = w_down.shape[1]
    ncols = vocab.shape[1]
    mine = (z * nx + x) * nc + c
    span = nz * own
    half = nx * span
    feats = nq * cols
    rows = -(-(units + own) // 16) * 16

    order = np.arange(group).reshape(nz, nq, own).transpose(1, 0, 2).reshape(-1)
    order = jnp.asarray(np.eye(group, dtype=np.float32)[order], bf16)
    mine_h = dot(hidden, order, 0, 1).astype(bf16)
    part = stream.reshape(own, nz, feats).transpose(1, 0, 2)
    part = jnp.pad(part, ((0, 0), (units, rows - units - own), (0, group - feats)))
    mine_h = jnp.pad(mine_h, ((0, rows - units), (0, 0)))
    first = exchange(mine_h[None] + part, Z)

    blocks = w_down.T.reshape(cols, nz, nq, units).transpose(2, 0, 1, 3)
    blocks = jnp.pad(blocks, ((0, 0), (0, 0), (0, 0), (0, rows - units)))
    blocks = blocks.reshape(nx, nc, cols, nz * rows).transpose(1, 0, 2, 3)
    kept, sent = halves(blocks, c)
    came = partner(sent, C, 1)
    pair = jnp.concatenate([jnp.where(c == 0, kept, came), jnp.where(c == 0, came, kept)], axis=0)
    pair = pair.transpose(1, 0, 2, 3)
    w_rows = jnp.zeros_like(pair)
    for step in range(nx):
        block = lax.dynamic_slice_in_dim(pair, x ^ step, 1)
        block = partner(block, X, step) if step else block
        w_rows = lax.dynamic_update_slice_in_dim(w_rows, block, x ^ step, 0)

    partial = dot(first.reshape(nz * rows, group), w_rows.reshape(feats, nz * rows), 0, 1)
    proj = jnp.sum(exchange(partial.reshape(nq, span, feats), Q), axis=0)
    row_part = first[:, units : units + own, :feats].reshape(span, feats)
    normin = (row_part.astype(f32) + proj).astype(bf16)
    normin = shared(normin, Z, nz).transpose(1, 0, 2).reshape(span, width)
    values = normin.astype(f32)
    inv = lax.rsqrt(jnp.mean(values * values, axis=1, keepdims=True) + norm_eps)
    normed = (values * inv * final_gain).astype(bf16)
    normed = shared(normed, X, nx).reshape(half, width)

    vocab, vocab_bias, _ = lax.optimization_barrier((vocab, vocab_bias, proj))
    vocab = (vocab, partner(vocab, C, 1))
    bias = (vocab_bias, partner(vocab_bias.reshape(2, -1), C, 1).reshape(-1))

    line = lax.broadcasted_iota(jnp.int32, (half, group), 0)
    token = (line // own) % nz * (nq * own) + line // span * (nc * own) + c * own + line % own
    goals = jnp.where(token == lax.broadcasted_iota(jnp.int32, (half, group), 1), targets[None, :], 0)
    goals = jnp.sum(goals, axis=1)
    ids = lax.broadcasted_iota(jnp.int32, (half, ncols), 1)
    hit = [ids + k * ncols == goals[:, None] for k in (mine, mine ^ 1)]
    scores = [dot(normed, v, 1, 0) + b for v, b in zip(vocab, bias)]
    top = jnp.maximum(jnp.max(scores[0], axis=1), jnp.max(scores[1], axis=1))
    total = sum(jnp.sum(jnp.exp(s - top[:, None]), axis=1) for s in scores)
    goal = sum(jnp.sum(jnp.where(h, s, 0.0), axis=1) for h, s in zip(hit, scores))
    stats = jnp.stack([top + jnp.log(total), goal])
    stats = merged(shared(stats, X, nx))
    stats = merged(shared(stats, Z, nz))
    lse, goal = stats
    losses = lse - goal + zloss_weight * lse * lse
    losses = lax.dynamic_slice_in_dim(losses, x * span + z * own, own)
    scale = 1.0 + 2.0 * zloss_weight * lse
    dscore = [
        (jnp.exp(s - lse[:, None]) * scale[:, None] - jnp.where(h, 1.0, 0.0)).astype(bf16)
        for s, h in zip(scores, hit)
    ]
    row_term = sum(dot(d, v, 1, 1) for d, v in zip(dscore, vocab)).astype(bf16)

    row_term, *dscore = lax.optimization_barrier((row_term, *dscore))
    feat_group = width // ny
    pieces = []
    for step in range(ny):
        piece = lax.dynamic_slice_in_dim(normed, (y ^ step) * feat_group, feat_group, 1)
        piece = jnp.concatenate([piece, *dscore], axis=1)
        pieces.append(partner(piece, "dp", step) if step else piece)
    pieces = jnp.concatenate(pieces)
    at = feat_group + ncols
    swapped = jnp.concatenate([pieces[:, :feat_group], pieces[:, at:]], axis=1)
    grad_vocab = sum(
        dot(p[:, :feat_group], p[:, feat_group:at], 0, 0) for p in (pieces, partner(swapped, C, 1))
    )

    row_x = exchange(row_term.reshape(nx, span, width), X)
    row_x = jnp.sum(row_x.astype(f32), axis=0).astype(bf16)
    row_z = exchange(row_x.reshape(nz, own, width), Z)
    dnormed = jnp.sum(row_z.astype(f32), axis=0)

    values = lax.dynamic_slice_in_dim(values, z * own, own)
    inv = lax.dynamic_slice_in_dim(inv, z * own, own)
    scaled = dnormed * final_gain
    grad_input = inv * (
        scaled - values * inv * inv * jnp.mean(values * scaled, axis=1, keepdims=True)
    )
    return (losses, grad_input, grad_vocab)


def solution(mesh):
    torus = Mesh(mesh.devices.reshape(16, 4, 2, mesh.shape["dp"]), ("vp_0", "vp_1", "vp_2", "dp"))
    return jax.shard_map(
        body,
        mesh=torus,
        in_specs=(P(DP_VP, None), P("dp", VP), P(None, VP), P(), P(None, VP), P(VP), P("dp")),
        out_specs=(P(DP_VP), P(DP_VP, None), P("dp", VP)),
        check_vma=False,
    )
```

```python
import jax
import jax.numpy as jnp
import numpy as np
from jax import lax
from jax.sharding import Mesh
from jax.sharding import PartitionSpec as P


Z, X, C = "vp_0", "vp_1", "vp_2"
Q = ("vp_1", "vp_2")
ZX = ("vp_0", "vp_1")
VP = ("vp_0", "vp_1", "vp_2")
DP_VP = ("dp", "vp_0", "vp_1", "vp_2")

norm_eps = 1e-06
zloss_weight = 0.001
f32 = jnp.float32
bf16 = jnp.bfloat16


def exchange(blocks, axes):
    return lax.all_to_all(blocks, axes, split_axis=0, concat_axis=0, tiled=True)


def shared(block, axes, count):
    return exchange(jnp.broadcast_to(block[None], (count, *block.shape)), axes)


def partner(array, axes, step):
    return lax.ppermute(array, axes, [(k, k ^ step) for k in range(lax.axis_size(axes))])


def dot(a, b, da, db):
    return lax.dot_general(a, b, (((da,), (db,)), ((), ())), preferred_element_type=f32)


def blocks_over_x(rows, x, span):
    blocks = [lax.dynamic_slice_in_dim(rows, (x ^ k) * span, span) for k in range(rows.shape[0] // span)]
    return [partner(b, X, k) if k else b for k, b in enumerate(blocks)]


def halves(array, core):
    first = lax.dynamic_slice_in_dim(array, core * (array.shape[0] // 2), array.shape[0] // 2)
    other = (1 - core) * (array.shape[0] // 2)
    return first, lax.dynamic_slice_in_dim(array, other, array.shape[0] // 2)


def body(stream, hidden, w_down, final_gain, vocab, vocab_bias, targets):
    nz, nx, nc, ny = (lax.axis_size(a) for a in (Z, X, C, "dp"))
    z, x, c, y = (lax.axis_index(a) for a in (Z, X, C, "dp"))
    nq = nx * nc
    own, width = stream.shape
    group, units = hidden.shape
    cols = w_down.shape[1]
    ncols = vocab.shape[1]
    mine = (z * nx + x) * nc + c
    span = nz * own
    half = nx * span
    feats = nq * cols
    rows = -(-(units + own) // 16) * 16

    order = np.arange(group).reshape(nz, nq, own).transpose(1, 0, 2).reshape(-1)
    order = jnp.asarray(np.eye(group, dtype=np.float32)[order], bf16)
    mine_h = dot(hidden, order, 0, 1).astype(bf16)
    part = stream.reshape(own, nz, feats).transpose(1, 0, 2)
    part = jnp.pad(part, ((0, 0), (units, rows - units - own), (0, group - feats)))
    mine_h = jnp.pad(mine_h, ((0, rows - units), (0, 0)))
    first = exchange(mine_h[None] + part, Z)

    blocks = w_down.T.reshape(cols, nz, nq, units).transpose(2, 0, 1, 3)
    blocks = jnp.pad(blocks, ((0, 0), (0, 0), (0, 0), (0, rows - units)))
    blocks = blocks.reshape(nx, nc, cols, nz * rows).transpose(1, 0, 2, 3)
    kept, sent = halves(blocks, c)
    came = partner(sent, C, 1)
    pair = jnp.concatenate([jnp.where(c == 0, kept, came), jnp.where(c == 0, came, kept)], axis=0)
    pair = pair.transpose(1, 0, 2, 3)
    w_rows = jnp.zeros_like(pair)
    for step in range(nx):
        block = lax.dynamic_slice_in_dim(pair, x ^ step, 1)
        block = partner(block, X, step) if step else block
        w_rows = lax.dynamic_update_slice_in_dim(w_rows, block, x ^ step, 0)

    partial = dot(first.reshape(nz * rows, group), w_rows.reshape(feats, nz * rows), 0, 1)

    vocab, vocab_bias, partial = lax.optimization_barrier((vocab, vocab_bias, partial))
    vocab = (vocab, partner(vocab, C, 1))
    bias = (vocab_bias, partner(vocab_bias.reshape(2, -1), C, 1).reshape(-1))
    line = lax.broadcasted_iota(jnp.int32, (half, group), 0)
    token = (line // own) % nz * (nq * own) + line // span * (nc * own) + c * own + line % own
    goals = jnp.where(token == lax.broadcasted_iota(jnp.int32, (half, group), 1), targets[None, :], 0)
    goals = jnp.sum(goals, axis=1)
    ids = lax.broadcasted_iota(jnp.int32, (half, ncols), 1)
    hit = [ids + k * ncols == goals[:, None] for k in (mine, mine ^ 1)]

    proj = jnp.sum(exchange(partial.reshape(nq, span, feats), Q), axis=0)
    row_part = first[:, units : units + own, :feats].reshape(span, feats)
    normin = (row_part.astype(f32) + proj).astype(bf16)
    goal_rows = sum(dot(h.astype(bf16), v, 1, 1) for h, v in zip(hit, vocab)).astype(bf16)
    goal_rows = blocks_over_x(goal_rows, x, span)
    normin, *goal_rows = lax.optimization_barrier((shared(normin, Z, nz), *goal_rows))
    goal_rows = sum(g.astype(f32) for g in goal_rows)
    normin = normin.transpose(1, 0, 2).reshape(span, width)
    values = normin.astype(f32)
    inv = lax.rsqrt(jnp.mean(values * values, axis=1, keepdims=True) + norm_eps)
    normed = (values * inv * final_gain).astype(bf16)
    normed = shared(normed, X, nx).reshape(half, width)

    scores = [dot(normed, v, 1, 0) + b for v, b in zip(vocab, bias)]
    top = jnp.maximum(jnp.max(scores[0], axis=1), jnp.max(scores[1], axis=1))
    total = sum(jnp.sum(jnp.exp(s - top[:, None]), axis=1) for s in scores)
    goal = sum(jnp.sum(jnp.where(h, s, 0.0), axis=1) for h, s in zip(hit, scores))
    local = top + jnp.log(total)
    stats = shared(jnp.stack([local, goal]), ZX, nz * nx)
    terms = sum(
        dot(jnp.where(h, 0.0, jnp.exp(s - local[:, None])).astype(bf16), v, 1, 1)
        for h, s, v in zip(hit, scores, vocab)
    ).astype(bf16)
    terms = blocks_over_x(terms, x, span)

    top = jnp.max(stats[:, 0], axis=0)
    lse = top + jnp.log(jnp.sum(jnp.exp(stats[:, 0] - top), axis=0))
    goal = jnp.sum(stats[:, 1], axis=0)
    losses = lse - goal + zloss_weight * lse * lse
    losses = lax.dynamic_slice_in_dim(losses, x * span + z * own, own)
    scale = 1.0 + 2.0 * zloss_weight * lse
    dscore = [
        (jnp.exp(s - lse[:, None]) * scale[:, None] - jnp.where(h, 1.0, 0.0)).astype(bf16)
        for s, h in zip(scores, hit)
    ]
    shares = jnp.concatenate([jnp.exp(stats[:, 0] - lse) * scale, (jnp.exp(goal - lse) * scale - 1.0)[None]])
    shares = lax.dynamic_slice_in_dim(shares, x * span, span, 1)
    row_x = shares[-1][:, None] * goal_rows
    for step in range(nx):
        share = lax.dynamic_slice_in_dim(shares, z * nx + (x ^ step), 1)
        row_x = row_x + share.reshape(span, 1) * terms[step].astype(f32)
    row_x = row_x.astype(bf16)

    row_x, *dscore = lax.optimization_barrier((row_x, *dscore))
    feat_group = width // ny
    pieces = []
    for step in range(ny):
        piece = lax.dynamic_slice_in_dim(normed, (y ^ step) * feat_group, feat_group, 1)
        piece = jnp.concatenate([piece, *dscore], axis=1)
        pieces.append(partner(piece, "dp", step) if step else piece)
    pieces = jnp.concatenate(pieces)
    at = feat_group + ncols
    theirs = dot(pieces[:, :feat_group], pieces[:, at:], 0, 0)
    grad_vocab = dot(pieces[:, :feat_group], pieces[:, feat_group:at], 0, 0) + partner(theirs, C, 1)

    row_z = exchange(row_x.reshape(nz, own, width), Z)
    dnormed = jnp.sum(row_z.astype(f32), axis=0)

    values = lax.dynamic_slice_in_dim(values, z * own, own)
    inv = lax.dynamic_slice_in_dim(inv, z * own, own)
    scaled = dnormed * final_gain
    grad_input = inv * (
        scaled - values * inv * inv * jnp.mean(values * scaled, axis=1, keepdims=True)
    )
    return (losses, grad_input, grad_vocab)


def solution(mesh):
    torus = Mesh(mesh.devices.reshape(16, 4, 2, mesh.shape["dp"]), ("vp_0", "vp_1", "vp_2", "dp"))
    return jax.shard_map(
        body,
        mesh=torus,
        in_specs=(P(DP_VP, None), P("dp", VP), P(None, VP), P(), P(None, VP), P(VP), P("dp")),
        out_specs=(P(DP_VP), P(DP_VP, None), P("dp", VP)),
        check_vma=False,
    )
```

```python
import jax
import jax.numpy as jnp
import numpy as np
from jax import lax
from jax.sharding import Mesh
from jax.sharding import PartitionSpec as P


Z, X, C = "vp_0", "vp_1", "vp_2"
Q = ("vp_1", "vp_2")
VP = ("vp_0", "vp_1", "vp_2")
DP_VP = ("dp", "vp_0", "vp_1", "vp_2")

norm_eps = 1e-06
zloss_weight = 0.001
f32 = jnp.float32
bf16 = jnp.bfloat16


def exchange(blocks, axes):
    return lax.all_to_all(blocks, axes, split_axis=0, concat_axis=0, tiled=True)


def shared(block, axes, count):
    return exchange(jnp.broadcast_to(block[None], (count, *block.shape)), axes)


def partner(array, axes, step):
    return lax.ppermute(array, axes, [(k, k ^ step) for k in range(lax.axis_size(axes))])


def dot(a, b, da, db):
    return lax.dot_general(a, b, (((da,), (db,)), ((), ())), preferred_element_type=f32)


def merged(stats):
    top = jnp.max(stats[:, 0], axis=0)
    lse = top + jnp.log(jnp.sum(jnp.exp(stats[:, 0] - top), axis=0))
    return jnp.stack([lse, jnp.sum(stats[:, 1], axis=0)])


def blocks_over_x(rows, x, span):
    blocks = [lax.dynamic_slice_in_dim(rows, (x ^ k) * span, span) for k in range(rows.shape[0] // span)]
    return [partner(b, X, k) if k else b for k, b in enumerate(blocks)]


def halves(array, core):
    first = lax.dynamic_slice_in_dim(array, core * (array.shape[0] // 2), array.shape[0] // 2)
    other = (1 - core) * (array.shape[0] // 2)
    return first, lax.dynamic_slice_in_dim(array, other, array.shape[0] // 2)


def body(stream, hidden, w_down, final_gain, vocab, vocab_bias, targets):
    nz, nx, nc, ny = (lax.axis_size(a) for a in (Z, X, C, "dp"))
    z, x, c, y = (lax.axis_index(a) for a in (Z, X, C, "dp"))
    nq = nx * nc
    own, width = stream.shape
    group, units = hidden.shape
    cols = w_down.shape[1]
    ncols = vocab.shape[1]
    mine = (z * nx + x) * nc + c
    span = nz * own
    half = nx * span
    feats = nq * cols
    rows = -(-(units + own) // 16) * 16

    order = np.arange(group).reshape(nz, nq, own).transpose(1, 0, 2).reshape(-1)
    order = jnp.asarray(np.eye(group, dtype=np.float32)[order], bf16)
    mine_h = dot(hidden, order, 0, 1).astype(bf16)
    part = stream.reshape(own, nz, feats).transpose(1, 0, 2)
    part = jnp.pad(part, ((0, 0), (units, rows - units - own), (0, group - feats)))
    mine_h = jnp.pad(mine_h, ((0, rows - units), (0, 0)))
    first = exchange(mine_h[None] + part, Z)

    blocks = w_down.T.reshape(cols, nz, nq, units).transpose(2, 0, 1, 3)
    blocks = jnp.pad(blocks, ((0, 0), (0, 0), (0, 0), (0, rows - units)))
    blocks = blocks.reshape(nx, nc, cols, nz * rows).transpose(1, 0, 2, 3)
    kept, sent = halves(blocks, c)
    came = partner(sent, C, 1)
    pair = jnp.concatenate([jnp.where(c == 0, kept, came), jnp.where(c == 0, came, kept)], axis=0)
    pair = pair.transpose(1, 0, 2, 3)
    w_rows = jnp.zeros_like(pair)
    for step in range(nx):
        block = lax.dynamic_slice_in_dim(pair, x ^ step, 1)
        block = partner(block, X, step) if step else block
        w_rows = lax.dynamic_update_slice_in_dim(w_rows, block, x ^ step, 0)

    partial = dot(first.reshape(nz * rows, group), w_rows.reshape(feats, nz * rows), 0, 1)

    vocab, vocab_bias, partial = lax.optimization_barrier((vocab, vocab_bias, partial))
    vocab = (vocab, partner(vocab, C, 1))
    bias = (vocab_bias, partner(vocab_bias.reshape(2, -1), C, 1).reshape(-1))
    line = lax.broadcasted_iota(jnp.int32, (half, group), 0)
    token = (line // own) % nz * (nq * own) + line // span * (nc * own) + c * own + line % own
    goals = jnp.where(token == lax.broadcasted_iota(jnp.int32, (half, group), 1), targets[None, :], 0)
    goals = jnp.sum(goals, axis=1)
    ids = lax.broadcasted_iota(jnp.int32, (half, ncols), 1)
    hit = [ids + k * ncols == goals[:, None] for k in (mine, mine ^ 1)]

    proj = jnp.sum(exchange(partial.reshape(nq, span, feats), Q), axis=0)
    row_part = first[:, units : units + own, :feats].reshape(span, feats)
    normin = (row_part.astype(f32) + proj).astype(bf16)
    goal_rows = sum(dot(h.astype(bf16), v, 1, 1) for h, v in zip(hit, vocab)).astype(bf16)
    goal_rows = blocks_over_x(goal_rows, x, span)
    normin, *goal_rows = lax.optimization_barrier((shared(normin, Z, nz), *goal_rows))
    goal_rows = sum(g.astype(f32) for g in goal_rows)
    normin = normin.transpose(1, 0, 2).reshape(span, width)
    values = normin.astype(f32)
    inv = lax.rsqrt(jnp.mean(values * values, axis=1, keepdims=True) + norm_eps)
    normed = (values * inv * final_gain).astype(bf16)
    normed = shared(normed, X, nx).reshape(half, width)

    feat_group, far = width // ny, ny // 2
    slices = [lax.dynamic_slice_in_dim(normed, (y ^ k) * feat_group, feat_group, 1) for k in range(ny)]
    slices[far] = partner(slices[far], "dp", far)

    scores = [dot(normed, v, 1, 0) + b for v, b in zip(vocab, bias)]
    top = jnp.maximum(jnp.max(scores[0], axis=1), jnp.max(scores[1], axis=1))
    total = sum(jnp.sum(jnp.exp(s - top[:, None]), axis=1) for s in scores)
    goal = sum(jnp.sum(jnp.where(h, s, 0.0), axis=1) for h, s in zip(hit, scores))
    local = top + jnp.log(total)
    near = shared(jnp.stack([local, goal]), X, nx)
    terms = sum(
        dot(jnp.where(h, 0.0, jnp.exp(s - local[:, None])).astype(bf16), v, 1, 1)
        for h, s, v in zip(hit, scores, vocab)
    ).astype(bf16)
    terms = blocks_over_x(terms, x, span)

    stats = shared(merged(near), Z, nz)
    lse, goal = merged(stats)
    losses = lse - goal + zloss_weight * lse * lse
    losses = lax.dynamic_slice_in_dim(losses, x * span + z * own, own)
    scale = 1.0 + 2.0 * zloss_weight * lse
    dscore = [
        (jnp.exp(s - lse[:, None]) * scale[:, None] - jnp.where(h, 1.0, 0.0)).astype(bf16)
        for s, h in zip(scores, hit)
    ]
    shares = jnp.concatenate([jnp.exp(near[:, 0] - lse) * scale, (jnp.exp(goal - lse) * scale - 1.0)[None]])
    shares = lax.dynamic_slice_in_dim(shares, x * span, span, 1)
    row_x = shares[-1][:, None] * goal_rows
    for step in range(nx):
        share = lax.dynamic_slice_in_dim(shares, x ^ step, 1)
        row_x = row_x + share.reshape(span, 1) * terms[step].astype(f32)
    row_x = row_x.astype(bf16)

    row_x, *dscore = lax.optimization_barrier((row_x, *dscore))
    theirs, ours = 0.0, 0.0
    for step in range(ny):
        piece, cols_of = slices[step], jnp.concatenate(dscore, axis=1)
        if step == far:
            cols_of = partner(cols_of, "dp", step)
        elif step:
            piece = partner(jnp.concatenate([piece, cols_of], axis=1), "dp", step)
            piece, cols_of = piece[:, :feat_group], piece[:, feat_group:]
        theirs = theirs + dot(piece, cols_of[:, ncols:], 0, 0)
        ours = ours + dot(piece, cols_of[:, :ncols], 0, 0)
    grad_vocab = lax.optimization_barrier(ours) + partner(theirs, C, 1)

    row_z = exchange(row_x.reshape(nz, own, width), Z)
    dnormed = jnp.sum(row_z.astype(f32), axis=0)

    values = lax.dynamic_slice_in_dim(values, z * own, own)
    inv = lax.dynamic_slice_in_dim(inv, z * own, own)
    scaled = dnormed * final_gain
    grad_input = inv * (
        scaled - values * inv * inv * jnp.mean(values * scaled, axis=1, keepdims=True)
    )
    return (losses, grad_input, grad_vocab)


def solution(mesh):
    torus = Mesh(mesh.devices.reshape(16, 4, 2, mesh.shape["dp"]), ("vp_0", "vp_1", "vp_2", "dp"))
    return jax.shard_map(
        body,
        mesh=torus,
        in_specs=(P(DP_VP, None), P("dp", VP), P(None, VP), P(), P(None, VP), P(VP), P("dp")),
        out_specs=(P(DP_VP), P(DP_VP, None), P("dp", VP)),
        check_vma=False,
    )
```

```python
import jax
import jax.numpy as jnp
import numpy as np
from jax import lax
from jax.experimental import pallas as pl
from jax.experimental.pallas import tpu as pltpu
from jax.sharding import Mesh
from jax.sharding import PartitionSpec as P


Z, X, C = "vp_0", "vp_1", "vp_2"
Q = ("vp_1", "vp_2")
VP = ("vp_0", "vp_1", "vp_2")
DP_VP = ("dp", "vp_0", "vp_1", "vp_2")

norm_eps = 1e-06
zloss_weight = 0.001
f32 = jnp.float32
bf16 = jnp.bfloat16


def exchange(blocks, axes):
    return lax.all_to_all(blocks, axes, split_axis=0, concat_axis=0, tiled=True)


def shared(block, axes, count):
    return exchange(jnp.broadcast_to(block[None], (count, *block.shape)), axes)


def partner(array, axes, step):
    return lax.ppermute(array, axes, [(k, k ^ step) for k in range(lax.axis_size(axes))])


def dot(a, b, da, db):
    return lax.dot_general(a, b, (((da,), (db,)), ((), ())), preferred_element_type=f32)


def merged(stats):
    top = jnp.max(stats[:, 0], axis=0)
    lse = top + jnp.log(jnp.sum(jnp.exp(stats[:, 0] - top), axis=0))
    return jnp.stack([lse, jnp.sum(stats[:, 1], axis=0)])


def halves(array, core):
    first = lax.dynamic_slice_in_dim(array, core * (array.shape[0] // 2), array.shape[0] // 2)
    other = (1 - core) * (array.shape[0] // 2)
    return first, lax.dynamic_slice_in_dim(array, other, array.shape[0] // 2)


def end_kernel(row_ref, values_ref, gain_ref, out_ref):
    values = values_ref[...]
    inv = lax.rsqrt(jnp.mean(values * values, axis=1, keepdims=True) + norm_eps)
    scaled = jnp.sum(row_ref[...].astype(f32), axis=0) * gain_ref[...]
    mean = jnp.mean(values * scaled, axis=1, keepdims=True)
    out_ref[...] = inv * (scaled - values * inv * inv * mean)


def body(stream, hidden, w_down, final_gain, vocab, vocab_bias, targets):
    nz, nx, nc, ny = (lax.axis_size(a) for a in (Z, X, C, "dp"))
    z, x, c, y = (lax.axis_index(a) for a in (Z, X, C, "dp"))
    nq = nx * nc
    own, width = stream.shape
    group, units = hidden.shape
    cols = w_down.shape[1]
    ncols = vocab.shape[1]
    mine = (z * nx + x) * nc + c
    span = nz * own
    half = nx * span
    feats = nq * cols
    rows = -(-(units + own) // 16) * 16

    order = np.arange(group).reshape(nz, nq, own).transpose(1, 0, 2).reshape(-1)
    order = jnp.asarray(np.eye(group, dtype=np.float32)[order], bf16)
    mine_h = hidden.T
    part = stream.reshape(own, nz, feats).transpose(1, 0, 2)
    part = jnp.pad(part, ((0, 0), (units, rows - units - own), (0, group - feats)))
    mine_h = jnp.pad(mine_h, ((0, rows - units), (0, 0)))
    first = exchange(mine_h[None] + part, Z)

    blocks = w_down.T.reshape(cols, nz, nq, units).transpose(2, 0, 1, 3)
    blocks = jnp.pad(blocks, ((0, 0), (0, 0), (0, 0), (0, rows - units)))
    blocks = blocks.reshape(nx, nc, cols, nz * rows).transpose(1, 0, 2, 3)
    kept, sent = halves(blocks, c)
    came = partner(sent, C, 1)
    pair = jnp.concatenate([jnp.where(c == 0, kept, came), jnp.where(c == 0, came, kept)], axis=0)
    pair = pair.transpose(1, 0, 2, 3)
    w_rows = jnp.zeros_like(pair)
    for step in range(nx):
        block = lax.dynamic_slice_in_dim(pair, x ^ step, 1)
        block = partner(block, X, step) if step else block
        w_rows = lax.dynamic_update_slice_in_dim(w_rows, block, x ^ step, 0)

    sorted_h = dot(order, first.reshape(nz * rows, group), 1, 1).astype(bf16)
    partial = dot(sorted_h, w_rows.reshape(feats, nz * rows), 1, 1)
    proj = jnp.sum(exchange(partial.reshape(nq, span, feats), Q), axis=0)
    first, proj = lax.optimization_barrier((first, proj))
    row_part = first[:, units : units + own, :feats].reshape(span, feats)
    normin = (row_part.astype(f32) + proj).astype(bf16)
    gathered = shared(normin, Z, nz)
    values = gathered.transpose(1, 0, 2).reshape(span, width).astype(f32)
    inv = lax.rsqrt(jnp.mean(values * values, axis=1, keepdims=True) + norm_eps)
    normed = (values * inv * final_gain).astype(bf16)
    normed = shared(normed, X, nx).reshape(half, width)

    vocab = (vocab, partner(vocab, C, 1))
    bias = (vocab_bias, partner(vocab_bias.reshape(2, -1), C, 1).reshape(-1))

    line = lax.broadcasted_iota(jnp.int32, (half, group), 0)
    token = (line // own) % nz * (nq * own) + line // span * (nc * own) + c * own + line % own
    goals = jnp.where(token == lax.broadcasted_iota(jnp.int32, (half, group), 1), targets[None, :], 0)
    goals = jnp.sum(goals, axis=1)
    ids = lax.broadcasted_iota(jnp.int32, (half, ncols), 1)
    hit = [ids + k * ncols == goals[:, None] for k in (mine, mine ^ 1)]
    feat_group, last = width // ny, ny - 1
    early = lax.dynamic_slice_in_dim(normed, (y ^ last) * feat_group, feat_group, 1)
    early = partner(early, "dp", last)

    scores = [dot(normed, v, 1, 0) + b for v, b in zip(vocab, bias)]
    top = jnp.maximum(jnp.max(scores[0], axis=1), jnp.max(scores[1], axis=1))
    total = sum(jnp.sum(jnp.exp(s - top[:, None]), axis=1) for s in scores)
    goal = sum(jnp.sum(jnp.where(h, s, 0.0), axis=1) for h, s in zip(hit, scores))
    stats = jnp.stack([top + jnp.log(total), goal])
    stats = merged(shared(stats, X, nx))
    stats = merged(shared(stats, Z, nz))
    lse, goal = stats
    losses = lse - goal + zloss_weight * lse * lse
    losses = lax.dynamic_slice_in_dim(losses, x * span + z * own, own)
    scale = 1.0 + 2.0 * zloss_weight * lse
    dscore = [
        (jnp.exp(s - lse[:, None]) * scale[:, None] - jnp.where(h, 1.0, 0.0)).astype(bf16)
        for s, h in zip(scores, hit)
    ]
    row_term = sum(dot(d, v, 1, 1) for d, v in zip(dscore, vocab)).astype(bf16)

    row_term, *dscore = lax.optimization_barrier((row_term, *dscore))
    theirs, ours = 0.0, 0.0
    for step in (0, ny // 2, 1, last):
        cols_of = jnp.concatenate(dscore, axis=1)
        if step == last:
            piece, cols_of = early, partner(cols_of, "dp", step)
        else:
            piece = lax.dynamic_slice_in_dim(normed, (y ^ step) * feat_group, feat_group, 1)
            if step:
                piece = partner(jnp.concatenate([piece, cols_of], axis=1), "dp", step)
                piece, cols_of = piece[:, :feat_group], piece[:, feat_group:]
        theirs = theirs + dot(piece, cols_of[:, ncols:], 0, 0)
        ours = ours + dot(piece, cols_of[:, :ncols], 0, 0)
    grad_vocab = lax.optimization_barrier(ours) + partner(theirs, C, 1)

    row_x = exchange(row_term.reshape(nx, span, width), X)
    row_x = jnp.sum(row_x.astype(f32), axis=0).astype(bf16)
    row_z = exchange(row_x.reshape(nz, own, width), Z)
    gathered, _ = lax.optimization_barrier((gathered, row_x))
    normin = lax.dynamic_slice_in_dim(gathered, z * own, own, 1).transpose(1, 0, 2).reshape(own, width)
    grad_input = pl.pallas_call(
        end_kernel,
        out_shape=jax.ShapeDtypeStruct((own, width), f32),
        in_specs=[pl.BlockSpec(memory_space=pltpu.VMEM)] * 3,
        out_specs=pl.BlockSpec(memory_space=pltpu.VMEM),
        compiler_params=pltpu.CompilerParams(vmem_limit_bytes=4 << 20),
    )(row_z, normin.astype(f32), final_gain[None])
    return (losses, grad_input, grad_vocab)


def solution(mesh):
    torus = Mesh(mesh.devices.reshape(16, 4, 2, mesh.shape["dp"]), ("vp_0", "vp_1", "vp_2", "dp"))
    return jax.shard_map(
        body,
        mesh=torus,
        in_specs=(P(DP_VP, None), P("dp", VP), P(None, VP), P(), P(None, VP), P(VP), P("dp")),
        out_specs=(P(DP_VP), P(DP_VP, None), P("dp", VP)),
        check_vma=False,
    )
```

```python
import jax
import jax.numpy as jnp
import numpy as np
from jax import lax
from jax.experimental import pallas as pl
from jax.experimental.pallas import tpu as pltpu
from jax.sharding import Mesh
from jax.sharding import PartitionSpec as P


Z, X, C = "vp_0", "vp_1", "vp_2"
Q = ("vp_1", "vp_2")
VP = ("vp_0", "vp_1", "vp_2")
DP_VP = ("dp", "vp_0", "vp_1", "vp_2")

norm_eps = 1e-06
zloss_weight = 0.001
f32 = jnp.float32
bf16 = jnp.bfloat16


def exchange(blocks, axes):
    return lax.all_to_all(blocks, axes, split_axis=0, concat_axis=0, tiled=True)


def shared(block, axes, count):
    return exchange(jnp.broadcast_to(block[None], (count, *block.shape)), axes)


def partner(array, axes, step):
    return lax.ppermute(array, axes, [(k, k ^ step) for k in range(lax.axis_size(axes))])


def dot(a, b, da, db):
    return lax.dot_general(a, b, (((da,), (db,)), ((), ())), preferred_element_type=f32)


def merged(stats):
    top = jnp.max(stats[:, 0], axis=0)
    lse = top + jnp.log(jnp.sum(jnp.exp(stats[:, 0] - top), axis=0))
    return jnp.stack([lse, jnp.sum(stats[:, 1], axis=0)])


def parts_of(array):
    parts = []
    for _ in range(3):
        part = lax.reduce_precision(array, 8, 7)
        parts.append(part.astype(bf16))
        array = array - part
    return jnp.stack(parts)


def halves(array, core):
    first = lax.dynamic_slice_in_dim(array, core * (array.shape[0] // 2), array.shape[0] // 2)
    other = (1 - core) * (array.shape[0] // 2)
    return first, lax.dynamic_slice_in_dim(array, other, array.shape[0] // 2)


def end_kernel(row_ref, values_ref, gain_ref, out_ref):
    values = values_ref[...]
    inv = lax.rsqrt(jnp.mean(values * values, axis=1, keepdims=True) + norm_eps)
    scaled = jnp.sum(row_ref[...].astype(f32), axis=0) * gain_ref[...]
    mean = jnp.mean(values * scaled, axis=1, keepdims=True)
    out_ref[...] = inv * (scaled - values * inv * inv * mean)


def body(stream, hidden, w_down, final_gain, vocab, vocab_bias, targets):
    nz, nx, nc, ny = (lax.axis_size(a) for a in (Z, X, C, "dp"))
    z, x, c, y = (lax.axis_index(a) for a in (Z, X, C, "dp"))
    nq = nx * nc
    own, width = stream.shape
    group, units = hidden.shape
    cols = w_down.shape[1]
    ncols = vocab.shape[1]
    mine = (z * nx + x) * nc + c
    span = nz * own
    half = nx * span
    feats = nq * cols
    rows = -(-(units + own) // 16) * 16

    order = np.arange(group).reshape(nz, nq, own).transpose(1, 0, 2).reshape(-1)
    order = jnp.asarray(np.eye(group, dtype=np.float32)[order], bf16)
    mine_h = hidden.T
    part = stream.reshape(own, nz, feats).transpose(1, 0, 2)
    part = jnp.pad(part, ((0, 0), (units, rows - units - own), (0, group - feats)))
    mine_h = jnp.pad(mine_h, ((0, rows - units), (0, 0)))
    first = exchange(mine_h[None] + part, Z)

    blocks = w_down.T.reshape(cols, nz, nq, units).transpose(2, 0, 1, 3)
    blocks = jnp.pad(blocks, ((0, 0), (0, 0), (0, 0), (0, rows - units)))
    blocks = blocks.reshape(nx, nc, cols, nz * rows).transpose(1, 0, 2, 3)
    kept, sent = halves(blocks, c)
    came = partner(sent, C, 1)
    pair = jnp.concatenate([jnp.where(c == 0, kept, came), jnp.where(c == 0, came, kept)], axis=0)
    pair = pair.transpose(1, 0, 2, 3)
    w_rows = jnp.zeros_like(pair)
    for step in range(nx):
        block = lax.dynamic_slice_in_dim(pair, x ^ step, 1)
        block = partner(block, X, step) if step else block
        w_rows = lax.dynamic_update_slice_in_dim(w_rows, block, x ^ step, 0)

    vocab = (vocab, partner(vocab, C, 1))
    bias = (vocab_bias, partner(vocab_bias.reshape(2, -1), C, 1).reshape(-1))

    line = lax.broadcasted_iota(jnp.int32, (half, group), 0)
    token = (line // own) % nz * (nq * own) + line // span * (nc * own) + c * own + line % own
    goals = jnp.where(token == lax.broadcasted_iota(jnp.int32, (half, group), 1), targets[None, :], 0)
    goals = jnp.sum(goals, axis=1)
    ids = lax.broadcasted_iota(jnp.int32, (half, ncols), 1)
    hit = [ids + k * ncols == goals[:, None] for k in (mine, mine ^ 1)]
    goal_rows = sum(dot(h.astype(bf16), v, 1, 1) for h, v in zip(hit, vocab)).astype(bf16)
    pieces = []
    for step in range(nx):
        piece = lax.dynamic_slice_in_dim(goal_rows, (x ^ step) * span, span)
        pieces.append(partner(piece, X, step) if step else piece)

    sorted_h = dot(order, first.reshape(nz * rows, group), 1, 1).astype(bf16)
    partial = dot(sorted_h, w_rows.reshape(feats, nz * rows), 1, 1)
    proj = jnp.sum(exchange(partial.reshape(nq, span, feats), Q), axis=0)
    first, proj = lax.optimization_barrier((first, proj))
    row_part = first[:, units : units + own, :feats].reshape(span, feats)
    normin = (row_part.astype(f32) + proj).astype(bf16)
    gathered = shared(normin, Z, nz)
    values = gathered.transpose(1, 0, 2).reshape(span, width).astype(f32)
    inv = lax.rsqrt(jnp.mean(values * values, axis=1, keepdims=True) + norm_eps)
    normed = (values * inv * final_gain).astype(bf16)
    normed = shared(normed, X, nx).reshape(half, width)

    feat_group, far, last = width // ny, ny // 2, ny - 1
    early = {}
    for step in (far, last):
        piece = lax.dynamic_slice_in_dim(normed, (y ^ step) * feat_group, feat_group, 1)
        early[step] = partner(piece, "dp", step)

    scores = [dot(normed, v, 1, 0) + b for v, b in zip(vocab, bias)]
    top = jnp.maximum(jnp.max(scores[0], axis=1), jnp.max(scores[1], axis=1))
    total = sum(jnp.sum(jnp.exp(s - top[:, None]), axis=1) for s in scores)
    goal = sum(jnp.sum(jnp.where(h, s, 0.0), axis=1) for h, s in zip(hit, scores))
    local = top + jnp.log(total)
    terms = sum(
        dot(jnp.where(h, 0.0, jnp.exp(s - local[:, None])).astype(bf16), v, 1, 1)
        for h, s, v in zip(hit, scores, vocab)
    ).astype(bf16)
    stats = parts_of(jnp.stack([local, goal])).reshape(6, half)
    stats = jnp.broadcast_to(jnp.pad(stats, ((0, span - 6), (0, 0)))[None], (nx, span, half))
    terms = exchange(jnp.concatenate([terms.reshape(nx, span, width), stats], axis=2), X)
    terms, *pieces = lax.optimization_barrier((terms, *pieces))
    goal_rows = sum(p.astype(f32) for p in pieces).astype(bf16)
    near = jnp.sum(terms[:, :6, width:].reshape(nx, 3, 2, half).astype(f32), axis=1)
    terms = terms[:, :, :width]
    stats = merged(shared(merged(near), Z, nz))
    lse, goal = stats
    losses = lse - goal + zloss_weight * lse * lse
    losses = lax.dynamic_slice_in_dim(losses, x * span + z * own, own)
    scale = 1.0 + 2.0 * zloss_weight * lse
    dscore = [
        (jnp.exp(s - lse[:, None]) * scale[:, None] - jnp.where(h, 1.0, 0.0)).astype(bf16)
        for s, h in zip(scores, hit)
    ]
    shares = jnp.concatenate([jnp.exp(near[:, 0] - lse) * scale, (jnp.exp(goal - lse) * scale - 1.0)[None]])
    shares = lax.dynamic_slice_in_dim(shares, x * span, span, 1)
    row_x = shares[-1][:, None] * goal_rows.astype(f32)
    row_x = (row_x + jnp.sum(shares[:-1, :, None] * terms.astype(f32), axis=0)).astype(bf16)

    row_x, *dscore = lax.optimization_barrier((row_x, *dscore))
    theirs, ours = 0.0, 0.0
    for step in (0, far, 1, last):
        cols_of = jnp.concatenate(dscore, axis=1)
        if step in early:
            piece, cols_of = early[step], partner(cols_of, "dp", step)
        else:
            piece = lax.dynamic_slice_in_dim(normed, (y ^ step) * feat_group, feat_group, 1)
            if step:
                piece = partner(jnp.concatenate([piece, cols_of], axis=1), "dp", step)
                piece, cols_of = piece[:, :feat_group], piece[:, feat_group:]
        theirs = theirs + dot(piece, cols_of[:, ncols:], 0, 0)
        ours = ours + dot(piece, cols_of[:, :ncols], 0, 0)
    grad_vocab = lax.optimization_barrier(ours) + partner(theirs, C, 1)

    row_z = exchange(row_x.reshape(nz, own, width), Z)
    gathered, _ = lax.optimization_barrier((gathered, row_x))
    normin = lax.dynamic_slice_in_dim(gathered, z * own, own, 1).transpose(1, 0, 2).reshape(own, width)
    grad_input = pl.pallas_call(
        end_kernel,
        out_shape=jax.ShapeDtypeStruct((own, width), f32),
        in_specs=[pl.BlockSpec(memory_space=pltpu.VMEM)] * 3,
        out_specs=pl.BlockSpec(memory_space=pltpu.VMEM),
        compiler_params=pltpu.CompilerParams(vmem_limit_bytes=4 << 20),
    )(row_z, normin.astype(f32), final_gain[None])
    return (losses, grad_input, grad_vocab)


def solution(mesh):
    torus = Mesh(mesh.devices.reshape(16, 4, 2, mesh.shape["dp"]), ("vp_0", "vp_1", "vp_2", "dp"))
    return jax.shard_map(
        body,
        mesh=torus,
        in_specs=(P(DP_VP, None), P("dp", VP), P(None, VP), P(), P(None, VP), P(VP), P("dp")),
        out_specs=(P(DP_VP), P(DP_VP, None), P("dp", VP)),
        check_vma=False,
    )
```

```python
import jax
import jax.numpy as jnp
import numpy as np
from jax import lax
from jax.experimental import pallas as pl
from jax.experimental.pallas import tpu as pltpu
from jax.sharding import Mesh
from jax.sharding import PartitionSpec as P


Z, X, C = "vp_0", "vp_1", "vp_2"
Q = ("vp_1", "vp_2")
VP = ("vp_0", "vp_1", "vp_2")
DP_VP = ("dp", "vp_0", "vp_1", "vp_2")

norm_eps = 1e-06
zloss_weight = 0.001
f32 = jnp.float32
bf16 = jnp.bfloat16


def exchange(blocks, axes):
    return lax.all_to_all(blocks, axes, split_axis=0, concat_axis=0, tiled=True)


def shared(block, axes, count):
    return exchange(jnp.broadcast_to(block[None], (count, *block.shape)), axes)


def partner(array, axes, step):
    return lax.ppermute(array, axes, [(k, k ^ step) for k in range(lax.axis_size(axes))])


def dot(a, b, da, db):
    return lax.dot_general(a, b, (((da,), (db,)), ((), ())), preferred_element_type=f32)


def merged(stats):
    top = jnp.max(stats[:, 0], axis=0)
    lse = top + jnp.log(jnp.sum(jnp.exp(stats[:, 0] - top), axis=0))
    return jnp.stack([lse, jnp.sum(stats[:, 1], axis=0)])


def halves(array, core):
    first = lax.dynamic_slice_in_dim(array, core * (array.shape[0] // 2), array.shape[0] // 2)
    other = (1 - core) * (array.shape[0] // 2)
    return first, lax.dynamic_slice_in_dim(array, other, array.shape[0] // 2)


def end_kernel(row_ref, values_ref, gain_ref, out_ref):
    values = values_ref[...]
    inv = lax.rsqrt(jnp.mean(values * values, axis=1, keepdims=True) + norm_eps)
    scaled = jnp.sum(row_ref[...].astype(f32), axis=0) * gain_ref[...]
    mean = jnp.mean(values * scaled, axis=1, keepdims=True)
    out_ref[...] = inv * (scaled - values * inv * inv * mean)


def head_kernel(base_ref, normed_ref, own_ref, other_ref, bias_ref, goals_ref, block_ref, scores_ref):
    ncols = own_ref.shape[1]
    blocks, span, wide = block_ref.shape
    half, width = normed_ref.shape
    vocab = (own_ref, other_ref)
    normed, goals = normed_ref[...], goals_ref[...]
    scores = [dot(normed, v[...], 1, 0) + bias_ref[k : k + 1] for k, v in enumerate(vocab)]
    ids = lax.broadcasted_iota(jnp.int32, (half, ncols), 1)
    hit = [ids + base_ref[k] == goals for k in range(2)]
    top = jnp.maximum(*(jnp.max(s, axis=1, keepdims=True) for s in scores))
    total = sum(jnp.sum(jnp.exp(s - top), axis=1, keepdims=True) for s in scores)
    goal = sum(jnp.sum(jnp.where(h, s, 0.0), axis=1, keepdims=True) for h, s in zip(hit, scores))
    local = top + jnp.log(total)
    weights = [jnp.where(h, 0.0, jnp.exp(s - local)).astype(bf16) for h, s in zip(hit, scores)]
    lane = lax.broadcasted_iota(jnp.int32, (half, wide - width), 1)
    parts = jnp.zeros((half, wide - width), f32)
    for k, column in enumerate((local, goal)):
        for place in range(3):
            part = column.astype(bf16).astype(f32)
            parts = jnp.where(lane == 2 * place + k, part, parts)
            column = column - part
    parts = parts.T[:span].astype(bf16)
    for k in range(2):
        scores_ref[k] = scores[k]
    for at in range(0, width, 512):
        terms = sum(dot(w, v[at : at + 512], 1, 1) for w, v in zip(weights, vocab)).astype(bf16)
        for k in range(blocks):
            block_ref[k, :, at : at + 512] = terms[k * span : (k + 1) * span]
    for k in range(blocks):
        block_ref[k, :, width:] = parts


def body(stream, hidden, w_down, final_gain, vocab, vocab_bias, targets):
    nz, nx, nc, ny = (lax.axis_size(a) for a in (Z, X, C, "dp"))
    z, x, c, y = (lax.axis_index(a) for a in (Z, X, C, "dp"))
    nq = nx * nc
    own, width = stream.shape
    group, units = hidden.shape
    cols = w_down.shape[1]
    ncols = vocab.shape[1]
    mine = (z * nx + x) * nc + c
    span = nz * own
    half = nx * span
    feats = nq * cols
    rows = -(-(units + own) // 16) * 16

    order = np.arange(group).reshape(nz, nq, own).transpose(1, 0, 2).reshape(-1)
    order = jnp.asarray(np.eye(group, dtype=np.float32)[order], bf16)
    mine_h = hidden.T
    part = stream.reshape(own, nz, feats).transpose(1, 0, 2)
    part = jnp.pad(part, ((0, 0), (units, rows - units - own), (0, group - feats)))
    mine_h = jnp.pad(mine_h, ((0, rows - units), (0, 0)))
    first = exchange(mine_h[None] + part, Z)

    blocks = w_down.T.reshape(cols, nz, nq, units).transpose(2, 0, 1, 3)
    blocks = jnp.pad(blocks, ((0, 0), (0, 0), (0, 0), (0, rows - units)))
    blocks = blocks.reshape(nx, nc, cols, nz * rows).transpose(1, 0, 2, 3)
    kept, sent = halves(blocks, c)
    came = partner(sent, C, 1)
    pair = jnp.concatenate([jnp.where(c == 0, kept, came), jnp.where(c == 0, came, kept)], axis=0)
    pair = pair.transpose(1, 0, 2, 3)
    w_rows = jnp.zeros_like(pair)
    for step in range(nx):
        block = lax.dynamic_slice_in_dim(pair, x ^ step, 1)
        block = partner(block, X, step) if step else block
        w_rows = lax.dynamic_update_slice_in_dim(w_rows, block, x ^ step, 0)

    vocab = (vocab, partner(vocab, C, 1))
    bias = (vocab_bias, partner(vocab_bias.reshape(2, -1), C, 1).reshape(-1))

    line = lax.broadcasted_iota(jnp.int32, (half, group), 0)
    token = (line // own) % nz * (nq * own) + line // span * (nc * own) + c * own + line % own
    goals = jnp.where(token == lax.broadcasted_iota(jnp.int32, (half, group), 1), targets[None, :], 0)
    goals = jnp.sum(goals, axis=1)
    ids = lax.broadcasted_iota(jnp.int32, (half, ncols), 1)
    hit = [ids + k * ncols == goals[:, None] for k in (mine, mine ^ 1)]
    goal_rows = sum(dot(h.astype(bf16), v, 1, 1) for h, v in zip(hit, vocab)).astype(bf16)
    pieces = []
    for step in range(nx):
        piece = lax.dynamic_slice_in_dim(goal_rows, (x ^ step) * span, span)
        pieces.append(partner(piece, X, step) if step else piece)

    sorted_h = dot(order, first.reshape(nz * rows, group), 1, 1).astype(bf16)
    partial = dot(sorted_h, w_rows.reshape(feats, nz * rows), 1, 1)
    proj = jnp.sum(exchange(partial.reshape(nq, span, feats), Q), axis=0)
    first, proj = lax.optimization_barrier((first, proj))
    row_part = first[:, units : units + own, :feats].reshape(span, feats)
    normin = (row_part.astype(f32) + proj).astype(bf16)
    gathered = shared(normin, Z, nz)
    values = gathered.transpose(1, 0, 2).reshape(span, width).astype(f32)
    inv = lax.rsqrt(jnp.mean(values * values, axis=1, keepdims=True) + norm_eps)
    normed = (values * inv * final_gain).astype(bf16)
    normed = shared(normed, X, nx).reshape(half, width)

    feat_group, far, last = width // ny, ny // 2, ny - 1
    early = {}
    for step in (far, last):
        piece = lax.dynamic_slice_in_dim(normed, (y ^ step) * feat_group, feat_group, 1)
        early[step] = partner(piece, "dp", step)

    vmem, smem = (pl.BlockSpec(memory_space=m) for m in (pltpu.VMEM, pltpu.SMEM))
    block, scores = pl.pallas_call(
        head_kernel,
        out_shape=(
            jax.ShapeDtypeStruct((nx, span, width + half), bf16),
            jax.ShapeDtypeStruct((2, half, ncols), f32),
        ),
        in_specs=[smem, vmem, vmem, vmem, vmem, vmem],
        out_specs=(vmem, vmem),
        compiler_params=pltpu.CompilerParams(vmem_limit_bytes=24 << 20),
        cost_estimate=pl.CostEstimate(
            flops=8 * half * ncols * width, bytes_accessed=8 * ncols * width, transcendentals=4 * half * ncols
        ),
    )(
        jnp.stack([mine * ncols, (mine ^ 1) * ncols]),
        normed,
        *vocab,
        jnp.stack(bias),
        goals[:, None],
    )
    terms = exchange(block, X)
    terms, *pieces = lax.optimization_barrier((terms, *pieces))
    goal_rows = sum(p.astype(f32) for p in pieces).astype(bf16)
    near = jnp.sum(terms[:, :6, width:].reshape(nx, 3, 2, half).astype(f32), axis=1)
    terms = terms[:, :, :width]
    stats = merged(shared(merged(near), Z, nz))
    lse, goal = stats
    losses = lse - goal + zloss_weight * lse * lse
    losses = lax.dynamic_slice_in_dim(losses, x * span + z * own, own)
    scale = 1.0 + 2.0 * zloss_weight * lse
    dscore = [
        (jnp.exp(s - lse[:, None]) * scale[:, None] - jnp.where(h, 1.0, 0.0)).astype(bf16)
        for s, h in zip(scores, hit)
    ]
    shares = lax.dynamic_slice_in_dim(jnp.exp(near[:, 0] - lse) * scale, x * span, span, 1)
    goal_share = lax.dynamic_slice_in_dim(jnp.exp(goal - lse) * scale - 1.0, x * span, span)
    row_x = jnp.sum(shares[:, :, None] * terms.astype(f32), axis=0)
    row_x = (row_x + goal_share[:, None] * goal_rows.astype(f32)).astype(bf16)

    row_x, *dscore = lax.optimization_barrier((row_x, *dscore))
    theirs, ours = 0.0, 0.0
    for step in (0, far, 1, last):
        cols_of = jnp.concatenate(dscore, axis=1)
        if step in early:
            piece, cols_of = early[step], partner(cols_of, "dp", step)
        else:
            piece = lax.dynamic_slice_in_dim(normed, (y ^ step) * feat_group, feat_group, 1)
            if step:
                piece = partner(jnp.concatenate([piece, cols_of], axis=1), "dp", step)
                piece, cols_of = piece[:, :feat_group], piece[:, feat_group:]
        theirs = theirs + dot(piece, cols_of[:, ncols:], 0, 0)
        ours = ours + dot(piece, cols_of[:, :ncols], 0, 0)
    grad_vocab = lax.optimization_barrier(ours) + partner(theirs, C, 1)

    row_z = exchange(row_x.reshape(nz, own, width), Z)
    gathered, _ = lax.optimization_barrier((gathered, row_x))
    normin = lax.dynamic_slice_in_dim(gathered, z * own, own, 1).transpose(1, 0, 2).reshape(own, width)
    grad_input = pl.pallas_call(
        end_kernel,
        out_shape=jax.ShapeDtypeStruct((own, width), f32),
        in_specs=[pl.BlockSpec(memory_space=pltpu.VMEM)] * 3,
        out_specs=pl.BlockSpec(memory_space=pltpu.VMEM),
        compiler_params=pltpu.CompilerParams(vmem_limit_bytes=4 << 20),
    )(row_z, normin.astype(f32), final_gain[None])
    return (losses, grad_input, grad_vocab)


def solution(mesh):
    torus = Mesh(mesh.devices.reshape(16, 4, 2, mesh.shape["dp"]), ("vp_0", "vp_1", "vp_2", "dp"))
    return jax.shard_map(
        body,
        mesh=torus,
        in_specs=(P(DP_VP, None), P("dp", VP), P(None, VP), P(), P(None, VP), P(VP), P("dp")),
        out_specs=(P(DP_VP), P(DP_VP, None), P("dp", VP)),
        check_vma=False,
    )
```

```python
import jax
import jax.numpy as jnp
import numpy as np
from jax import lax
from jax.experimental import pallas as pl
from jax.experimental.pallas import tpu as pltpu
from jax.sharding import Mesh
from jax.sharding import PartitionSpec as P


Z, X, C = "vp_0", "vp_1", "vp_2"
Q = ("vp_1", "vp_2")
VP = ("vp_0", "vp_1", "vp_2")
DP_VP = ("dp", "vp_0", "vp_1", "vp_2")

norm_eps = 1e-06
zloss_weight = 0.001
f32 = jnp.float32
bf16 = jnp.bfloat16


def exchange(blocks, axes):
    return lax.all_to_all(blocks, axes, split_axis=0, concat_axis=0, tiled=True)


def shared(block, axes, count):
    return exchange(jnp.broadcast_to(block[None], (count, *block.shape)), axes)


def partner(array, axes, step):
    return lax.ppermute(array, axes, [(k, k ^ step) for k in range(lax.axis_size(axes))])


def dot(a, b, da, db):
    return lax.dot_general(a, b, (((da,), (db,)), ((), ())), preferred_element_type=f32)


def merged(stats):
    top = jnp.max(stats[:, 0], axis=0)
    lse = top + jnp.log(jnp.sum(jnp.exp(stats[:, 0] - top), axis=0))
    return jnp.stack([lse, jnp.sum(stats[:, 1], axis=0)])


def halves(array, core):
    first = lax.dynamic_slice_in_dim(array, core * (array.shape[0] // 2), array.shape[0] // 2)
    other = (1 - core) * (array.shape[0] // 2)
    return first, lax.dynamic_slice_in_dim(array, other, array.shape[0] // 2)


def end_kernel(row_ref, values_ref, gain_ref, out_ref):
    values = values_ref[...]
    inv = lax.rsqrt(jnp.mean(values * values, axis=1, keepdims=True) + norm_eps)
    scaled = jnp.sum(row_ref[...].astype(f32), axis=0) * gain_ref[...]
    mean = jnp.mean(values * scaled, axis=1, keepdims=True)
    out_ref[...] = inv * (scaled - values * inv * inv * mean)


def head_kernel(base_ref, normed_ref, own_ref, other_ref, bias_ref, goals_ref, stats_ref, scores_ref):
    half, ncols = normed_ref.shape[0], own_ref.shape[1]
    vocab = (own_ref, other_ref)
    normed, goals = normed_ref[...], goals_ref[...]
    scores = [dot(normed, v[...], 1, 0) + bias_ref[k : k + 1] for k, v in enumerate(vocab)]
    ids = lax.broadcasted_iota(jnp.int32, (half, ncols), 1)
    hit = [ids + base_ref[k] == goals for k in range(2)]
    top = jnp.maximum(*(jnp.max(s, axis=1, keepdims=True) for s in scores))
    total = sum(jnp.sum(jnp.exp(s - top), axis=1, keepdims=True) for s in scores)
    goal = sum(jnp.sum(jnp.where(h, s, 0.0), axis=1, keepdims=True) for h, s in zip(hit, scores))
    lane = lax.broadcasted_iota(jnp.int32, (half, half), 1)
    both = jnp.where(lane == 0, top + jnp.log(total), jnp.where(lane == 1, goal, 0.0)).T[:2]
    for k in range(stats_ref.shape[0]):
        stats_ref[k] = both
    for k in range(2):
        scores_ref[k] = scores[k]


def rows_kernel(base_ref, stats_ref, scores_ref, own_ref, other_ref, goals_ref, block_ref, dscore_ref, losses_ref):
    ncols = own_ref.shape[1]
    blocks, span, width = block_ref.shape
    half = blocks * span
    stats = stats_ref[...]
    tops = jnp.max(stats, axis=0)
    lse = tops + jnp.log(jnp.sum(jnp.exp(stats - tops), axis=0))
    lse, goal = lse[:1], jnp.sum(stats, axis=0)[1:]
    losses_ref[...] = lse - goal + zloss_weight * lse * lse
    lse = jnp.broadcast_to(lse, (half, half)).T[:, :1]
    scale = 1.0 + 2.0 * zloss_weight * lse
    ids = lax.broadcasted_iota(jnp.int32, (half, ncols), 1)
    dscore = []
    for k in range(2):
        hit = ids + base_ref[k] == goals_ref[...]
        d = jnp.exp(scores_ref[k] - lse) * scale - jnp.where(hit, 1.0, 0.0)
        dscore.append(d.astype(bf16))
        dscore_ref[:, k * ncols : (k + 1) * ncols] = dscore[k]
    for at in range(0, width, 512):
        terms = sum(dot(d, v[at : at + 512], 1, 1) for d, v in zip(dscore, (own_ref, other_ref))).astype(bf16)
        for k in range(blocks):
            block_ref[k, :, at : at + 512] = terms[k * span : (k + 1) * span]


def body(stream, hidden, w_down, final_gain, vocab, vocab_bias, targets):
    nz, nx, nc, ny = (lax.axis_size(a) for a in (Z, X, C, "dp"))
    z, x, c, y = (lax.axis_index(a) for a in (Z, X, C, "dp"))
    nq = nx * nc
    own, width = stream.shape
    group, units = hidden.shape
    cols = w_down.shape[1]
    ncols = vocab.shape[1]
    mine = (z * nx + x) * nc + c
    span = nz * own
    half = nx * span
    feats = nq * cols
    rows = -(-(units + own) // 16) * 16

    order = np.arange(group).reshape(nz, nq, own).transpose(1, 0, 2).reshape(-1)
    order = jnp.asarray(np.eye(group, dtype=np.float32)[order], bf16)
    mine_h = hidden.T
    part = stream.reshape(own, nz, feats).transpose(1, 0, 2)
    part = jnp.pad(part, ((0, 0), (units, rows - units - own), (0, group - feats)))
    mine_h = jnp.pad(mine_h, ((0, rows - units), (0, 0)))
    first = exchange(mine_h[None] + part, Z)

    blocks = w_down.T.reshape(cols, nz, nq, units).transpose(2, 0, 1, 3)
    blocks = jnp.pad(blocks, ((0, 0), (0, 0), (0, 0), (0, rows - units)))
    blocks = blocks.reshape(nx, nc, cols, nz * rows).transpose(1, 0, 2, 3)
    kept, sent = halves(blocks, c)
    came = partner(sent, C, 1)
    pair = jnp.concatenate([jnp.where(c == 0, kept, came), jnp.where(c == 0, came, kept)], axis=0)
    pair = pair.transpose(1, 0, 2, 3)
    w_rows = jnp.zeros_like(pair)
    for step in range(nx):
        block = lax.dynamic_slice_in_dim(pair, x ^ step, 1)
        block = partner(block, X, step) if step else block
        w_rows = lax.dynamic_update_slice_in_dim(w_rows, block, x ^ step, 0)

    sorted_h = dot(order, first.reshape(nz * rows, group), 1, 1).astype(bf16)
    partial = dot(sorted_h, w_rows.reshape(feats, nz * rows), 1, 1)
    proj = jnp.sum(exchange(partial.reshape(nq, span, feats), Q), axis=0)
    first, proj = lax.optimization_barrier((first, proj))
    row_part = first[:, units : units + own, :feats].reshape(span, feats)
    normin = (row_part.astype(f32) + proj).astype(bf16)
    gathered = shared(normin, Z, nz)
    values = gathered.transpose(1, 0, 2).reshape(span, width).astype(f32)
    inv = lax.rsqrt(jnp.mean(values * values, axis=1, keepdims=True) + norm_eps)
    normed = (values * inv * final_gain).astype(bf16)
    normed = shared(normed, X, nx).reshape(half, width)

    vocab = (vocab, partner(vocab, C, 1))
    bias = (vocab_bias, partner(vocab_bias.reshape(2, -1), C, 1).reshape(-1))

    line = lax.broadcasted_iota(jnp.int32, (half, group), 0)
    token = (line // own) % nz * (nq * own) + line // span * (nc * own) + c * own + line % own
    goals = jnp.where(token == lax.broadcasted_iota(jnp.int32, (half, group), 1), targets[None, :], 0)
    goals = jnp.sum(goals, axis=1)
    feat_group, last = width // ny, ny - 1
    early = lax.dynamic_slice_in_dim(normed, (y ^ last) * feat_group, feat_group, 1)
    early = partner(early, "dp", last)

    vmem, smem = (pl.BlockSpec(memory_space=m) for m in (pltpu.VMEM, pltpu.SMEM))
    base, goals = jnp.stack([mine * ncols, (mine ^ 1) * ncols]), goals[:, None]
    params = pltpu.CompilerParams(vmem_limit_bytes=24 << 20)
    cost = pl.CostEstimate(
        flops=4 * half * ncols * width, bytes_accessed=4 * ncols * width, transcendentals=2 * half * ncols
    )
    stats, scores = pl.pallas_call(
        head_kernel,
        out_shape=(
            jax.ShapeDtypeStruct((nx, 2, half), f32),
            jax.ShapeDtypeStruct((2, half, ncols), f32),
        ),
        in_specs=[smem] + [vmem] * 5,
        out_specs=(vmem,) * 2,
        compiler_params=params,
        cost_estimate=cost,
    )(base, normed, *vocab, jnp.stack(bias), goals)
    stats = merged(exchange(stats, X))
    stats = shared(stats, Z, nz)
    row_term, dscore, losses = pl.pallas_call(
        rows_kernel,
        out_shape=(
            jax.ShapeDtypeStruct((nx, span, width), bf16),
            jax.ShapeDtypeStruct((half, 2 * ncols), bf16),
            jax.ShapeDtypeStruct((1, half), f32),
        ),
        in_specs=[smem] + [vmem] * 5,
        out_specs=(vmem,) * 3,
        compiler_params=params,
        cost_estimate=cost,
    )(base, stats, scores, *vocab, goals)
    row_term, dscore, losses = lax.optimization_barrier((row_term, dscore, losses))
    losses = lax.dynamic_slice_in_dim(losses[0], x * span + z * own, own)

    row_x = exchange(row_term, X)
    row_x = jnp.sum(row_x.astype(f32), axis=0).astype(bf16)
    early, row_x = lax.optimization_barrier((early, row_x))
    early = lax.optimization_barrier(jnp.where(c >= 0, early, 0))
    theirs, ours = 0.0, 0.0
    for step in (0, ny // 2, 1, last):
        if step == last:
            piece, cols_of = early, partner(dscore, "dp", step)
        else:
            piece, cols_of = lax.dynamic_slice_in_dim(normed, (y ^ step) * feat_group, feat_group, 1), dscore
            if step:
                piece = partner(jnp.concatenate([piece, cols_of], axis=1), "dp", step)
                piece, cols_of = piece[:, :feat_group], piece[:, feat_group:]
        theirs = theirs + dot(piece, cols_of[:, ncols:], 0, 0)
        ours = ours + dot(piece, cols_of[:, :ncols], 0, 0)
    grad_vocab = lax.optimization_barrier(ours) + partner(theirs, C, 1)

    row_z = exchange(row_x.reshape(nz, own, width), Z)
    gathered, _ = lax.optimization_barrier((gathered, row_x))
    normin = lax.dynamic_slice_in_dim(gathered, z * own, own, 1).transpose(1, 0, 2).reshape(own, width)
    grad_input = pl.pallas_call(
        end_kernel,
        out_shape=jax.ShapeDtypeStruct((own, width), f32),
        in_specs=[pl.BlockSpec(memory_space=pltpu.VMEM)] * 3,
        out_specs=pl.BlockSpec(memory_space=pltpu.VMEM),
        compiler_params=pltpu.CompilerParams(vmem_limit_bytes=4 << 20),
    )(row_z, normin.astype(f32), final_gain[None])
    return (losses, grad_input, grad_vocab)


def solution(mesh):
    torus = Mesh(mesh.devices.reshape(16, 4, 2, mesh.shape["dp"]), ("vp_0", "vp_1", "vp_2", "dp"))
    return jax.shard_map(
        body,
        mesh=torus,
        in_specs=(P(DP_VP, None), P("dp", VP), P(None, VP), P(), P(None, VP), P(VP), P("dp")),
        out_specs=(P(DP_VP), P(DP_VP, None), P("dp", VP)),
        check_vma=False,
    )
```

```python
import jax
import jax.numpy as jnp
import numpy as np
from jax import lax
from jax.experimental import pallas as pl
from jax.experimental.pallas import tpu as pltpu
from jax.sharding import Mesh
from jax.sharding import PartitionSpec as P


Z, X, C = "vp_0", "vp_1", "vp_2"
Q = ("vp_1", "vp_2")
VP = ("vp_0", "vp_1", "vp_2")
DP_VP = ("dp", "vp_0", "vp_1", "vp_2")

norm_eps = 1e-06
zloss_weight = 0.001
f32 = jnp.float32
bf16 = jnp.bfloat16


def exchange(blocks, axes):
    return lax.all_to_all(blocks, axes, split_axis=0, concat_axis=0, tiled=True)


def shared(block, axes, count):
    return exchange(jnp.broadcast_to(block[None], (count, *block.shape)), axes)


def partner(array, axes, step):
    return lax.ppermute(array, axes, [(k, k ^ step) for k in range(lax.axis_size(axes))])


def dot(a, b, da, db):
    return lax.dot_general(a, b, (((da,), (db,)), ((), ())), preferred_element_type=f32)


def merged(stats):
    top = jnp.max(stats[:, 0], axis=0)
    lse = top + jnp.log(jnp.sum(jnp.exp(stats[:, 0] - top), axis=0))
    return jnp.stack([lse, jnp.sum(stats[:, 1], axis=0)])


def halves(array, core):
    first = lax.dynamic_slice_in_dim(array, core * (array.shape[0] // 2), array.shape[0] // 2)
    other = (1 - core) * (array.shape[0] // 2)
    return first, lax.dynamic_slice_in_dim(array, other, array.shape[0] // 2)


def end_kernel(row_ref, values_ref, gain_ref, out_ref):
    values = values_ref[...]
    inv = lax.rsqrt(jnp.mean(values * values, axis=1, keepdims=True) + norm_eps)
    scaled = jnp.sum(row_ref[...].astype(f32), axis=0) * gain_ref[...]
    mean = jnp.mean(values * scaled, axis=1, keepdims=True)
    out_ref[...] = inv * (scaled - values * inv * inv * mean)


def head_kernel(base_ref, normed_ref, own_ref, other_ref, bias_ref, goals_ref, stats_ref, scores_ref):
    half, ncols = normed_ref.shape[0], own_ref.shape[1]
    vocab = (own_ref, other_ref)
    normed, goals = normed_ref[...], goals_ref[...]
    scores = [dot(normed, v[...], 1, 0) + bias_ref[k : k + 1] for k, v in enumerate(vocab)]
    ids = lax.broadcasted_iota(jnp.int32, (half, ncols), 1)
    hit = [ids + base_ref[k] == goals for k in range(2)]
    top = jnp.maximum(*(jnp.max(s, axis=1, keepdims=True) for s in scores))
    total = sum(jnp.sum(jnp.exp(s - top), axis=1, keepdims=True) for s in scores)
    goal = sum(jnp.sum(jnp.where(h, s, 0.0), axis=1, keepdims=True) for h, s in zip(hit, scores))
    lane = lax.broadcasted_iota(jnp.int32, (half, half), 1)
    both = jnp.where(lane == 0, top + jnp.log(total), jnp.where(lane == 1, goal, 0.0)).T[:2]
    for k in range(stats_ref.shape[0]):
        stats_ref[k] = both
    for k in range(2):
        scores_ref[k] = scores[k]


def rows_kernel(base_ref, stats_ref, scores_ref, own_ref, other_ref, goals_ref, block_ref, dscore_ref, losses_ref):
    ncols = own_ref.shape[1]
    blocks, span, width = block_ref.shape
    half = blocks * span
    stats = stats_ref[...]
    tops = jnp.max(stats, axis=0)
    lse = tops + jnp.log(jnp.sum(jnp.exp(stats - tops), axis=0))
    lse, goal = lse[:1], jnp.sum(stats, axis=0)[1:]
    losses_ref[...] = lse - goal + zloss_weight * lse * lse
    lse = jnp.broadcast_to(lse, (half, half)).T[:, :1]
    scale = 1.0 + 2.0 * zloss_weight * lse
    ids = lax.broadcasted_iota(jnp.int32, (half, ncols), 1)
    dscore = []
    for k in range(2):
        hit = ids + base_ref[k] == goals_ref[...]
        d = jnp.exp(scores_ref[k] - lse) * scale - jnp.where(hit, 1.0, 0.0)
        dscore.append(d.astype(bf16))
        dscore_ref[:, k * ncols : (k + 1) * ncols] = dscore[k]
    for at in range(0, width, 512):
        terms = sum(dot(d, v[at : at + 512], 1, 1) for d, v in zip(dscore, (own_ref, other_ref))).astype(bf16)
        for k in range(blocks):
            block_ref[k, :, at : at + 512] = terms[k * span : (k + 1) * span]


def body(stream, hidden, w_down, final_gain, vocab, vocab_bias, targets):
    nz, nx, nc, ny = (lax.axis_size(a) for a in (Z, X, C, "dp"))
    z, x, c, y = (lax.axis_index(a) for a in (Z, X, C, "dp"))
    nq = nx * nc
    own, width = stream.shape
    group, units = hidden.shape
    cols = w_down.shape[1]
    ncols = vocab.shape[1]
    mine = (z * nx + x) * nc + c
    span = nz * own
    half = nx * span
    feats = nq * cols
    rows = -(-(units + own) // 16) * 16

    order = np.arange(group).reshape(nz, nq, own).transpose(1, 0, 2).reshape(-1)
    order = jnp.asarray(np.eye(group, dtype=np.float32)[order], bf16)
    mine_h = hidden.T
    part = stream.reshape(own, nz, feats).transpose(1, 0, 2)
    part = jnp.pad(part, ((0, 0), (units, rows - units - own), (0, group - feats)))
    mine_h = jnp.pad(mine_h, ((0, rows - units), (0, 0)))
    first = exchange(mine_h[None] + part, Z)

    blocks = w_down.T.reshape(cols, nz, nq, units).transpose(2, 0, 1, 3)
    blocks = jnp.pad(blocks, ((0, 0), (0, 0), (0, 0), (0, rows - units)))
    blocks = blocks.reshape(nx, nc, cols, nz * rows).transpose(1, 0, 2, 3)
    kept, sent = halves(blocks, c)
    came = partner(sent, C, 1)
    pair = jnp.concatenate([jnp.where(c == 0, kept, came), jnp.where(c == 0, came, kept)], axis=0)
    pair = pair.transpose(1, 0, 2, 3)
    w_rows = jnp.zeros_like(pair)
    for step in range(nx):
        block = lax.dynamic_slice_in_dim(pair, x ^ step, 1)
        block = partner(block, X, step) if step else block
        w_rows = lax.dynamic_update_slice_in_dim(w_rows, block, x ^ step, 0)

    sorted_h = dot(order, first.reshape(nz * rows, group), 1, 1).astype(bf16)
    partial = dot(sorted_h, w_rows.reshape(feats, nz * rows), 1, 1)
    proj = jnp.sum(exchange(partial.reshape(nq, span, feats), Q), axis=0)
    first, proj = lax.optimization_barrier((first, proj))
    row_part = first[:, units : units + own, :feats].reshape(span, feats)
    normin = (row_part.astype(f32) + proj).astype(bf16)
    gathered = shared(normin, Z, nz)
    values = gathered.transpose(1, 0, 2).reshape(span, width).astype(f32)
    inv = lax.rsqrt(jnp.mean(values * values, axis=1, keepdims=True) + norm_eps)
    normed = (values * inv * final_gain).astype(bf16)
    normed = shared(normed, X, nx).reshape(half, width)

    vocab = (vocab, partner(vocab, C, 1))
    bias = (vocab_bias, partner(vocab_bias.reshape(2, -1), C, 1).reshape(-1))

    line = lax.broadcasted_iota(jnp.int32, (half, group), 0)
    token = (line // own) % nz * (nq * own) + line // span * (nc * own) + c * own + line % own
    goals = jnp.where(token == lax.broadcasted_iota(jnp.int32, (half, group), 1), targets[None, :], 0)
    goals = jnp.sum(goals, axis=1)
    feat_group, last = width // ny, ny - 1
    early = lax.dynamic_slice_in_dim(normed, (y ^ last) * feat_group, feat_group, 1)
    early = partner(early, "dp", last)

    vmem, smem = (pl.BlockSpec(memory_space=m) for m in (pltpu.VMEM, pltpu.SMEM))
    base, goals = jnp.stack([mine * ncols, (mine ^ 1) * ncols]), goals[:, None]
    params = pltpu.CompilerParams(vmem_limit_bytes=24 << 20)
    cost = pl.CostEstimate(
        flops=4 * half * ncols * width, bytes_accessed=4 * ncols * width, transcendentals=2 * half * ncols
    )
    stats, scores = pl.pallas_call(
        head_kernel,
        out_shape=(
            jax.ShapeDtypeStruct((nx, 2, half), f32),
            jax.ShapeDtypeStruct((2, half, ncols), f32),
        ),
        in_specs=[smem] + [vmem] * 5,
        out_specs=(vmem,) * 2,
        compiler_params=params,
        cost_estimate=cost,
    )(base, normed, *vocab, jnp.stack(bias), goals)
    stats = merged(exchange(stats, X))
    stats = shared(stats, Z, nz)
    row_term, dscore, losses = pl.pallas_call(
        rows_kernel,
        out_shape=(
            jax.ShapeDtypeStruct((nx, span, width), bf16),
            jax.ShapeDtypeStruct((half, 2 * ncols), bf16),
            jax.ShapeDtypeStruct((1, half), f32),
        ),
        in_specs=[smem] + [vmem] * 5,
        out_specs=(vmem,) * 3,
        compiler_params=params,
        cost_estimate=cost,
    )(base, stats, scores, *vocab, goals)
    row_term, dscore, losses = lax.optimization_barrier((row_term, dscore, losses))
    losses = lax.dynamic_slice_in_dim(losses[0], x * span + z * own, own)

    row_x = exchange(row_term, X)
    row_x = jnp.sum(row_x.astype(f32), axis=0).astype(bf16)
    early, row_x = lax.optimization_barrier((early, row_x))
    early = jnp.where(c >= 0, early, 0)
    early = lax.optimization_barrier(early)
    theirs, ours = 0.0, 0.0
    for step in (0, ny // 2, 1, last):
        if step == last:
            piece, cols_of = early, partner(dscore, "dp", step)
        else:
            piece, cols_of = lax.dynamic_slice_in_dim(normed, (y ^ step) * feat_group, feat_group, 1), dscore
            if step:
                piece = partner(jnp.concatenate([piece, cols_of], axis=1), "dp", step)
                piece, cols_of = piece[:, :feat_group], piece[:, feat_group:]
        theirs = theirs + dot(piece, cols_of[:, ncols:], 0, 0)
        ours = ours + dot(piece, cols_of[:, :ncols], 0, 0)
    theirs = partner(theirs, C, 1)
    ours = lax.optimization_barrier(ours)
    grad_vocab = ours + theirs

    row_z = exchange(row_x.reshape(nz, own, width), Z)
    gathered, _ = lax.optimization_barrier((gathered, row_x))
    normin = lax.dynamic_slice_in_dim(gathered, z * own, own, 1).transpose(1, 0, 2).reshape(own, width)
    grad_input = pl.pallas_call(
        end_kernel,
        out_shape=jax.ShapeDtypeStruct((own, width), f32),
        in_specs=[pl.BlockSpec(memory_space=pltpu.VMEM)] * 3,
        out_specs=pl.BlockSpec(memory_space=pltpu.VMEM),
        compiler_params=pltpu.CompilerParams(vmem_limit_bytes=4 << 20),
    )(row_z, normin.astype(f32), final_gain[None])
    return (losses, grad_input, grad_vocab)


def solution(mesh):
    torus = Mesh(mesh.devices.reshape(16, 4, 2, mesh.shape["dp"]), ("vp_0", "vp_1", "vp_2", "dp"))
    return jax.shard_map(
        body,
        mesh=torus,
        in_specs=(P(DP_VP, None), P("dp", VP), P(None, VP), P(), P(None, VP), P(VP), P("dp")),
        out_specs=(P(DP_VP), P(DP_VP, None), P("dp", VP)),
        check_vma=False,
    )
```

```python
import jax
import jax.numpy as jnp
import numpy as np
from jax import lax
from jax.experimental import pallas as pl
from jax.experimental.pallas import tpu as pltpu
from jax.sharding import Mesh
from jax.sharding import PartitionSpec as P


Z, X, C = "vp_0", "vp_1", "vp_2"
Q = ("vp_1", "vp_2")
VP = ("vp_0", "vp_1", "vp_2")
DP_VP = ("dp", "vp_0", "vp_1", "vp_2")

norm_eps = 1e-06
zloss_weight = 0.001
f32 = jnp.float32
bf16 = jnp.bfloat16


def exchange(blocks, axes):
    return lax.all_to_all(blocks, axes, split_axis=0, concat_axis=0, tiled=True)


def shared(block, axes, count):
    return exchange(jnp.broadcast_to(block[None], (count, *block.shape)), axes)


def partner(array, axes, step):
    return lax.ppermute(array, axes, [(k, k ^ step) for k in range(lax.axis_size(axes))])


def dot(a, b, da, db):
    return lax.dot_general(a, b, (((da,), (db,)), ((), ())), preferred_element_type=f32)


def merged(stats):
    top = jnp.max(stats[:, 0], axis=0)
    lse = top + jnp.log(jnp.sum(jnp.exp(stats[:, 0] - top), axis=0))
    return jnp.stack([lse, jnp.sum(stats[:, 1], axis=0)])


def halves(array, core):
    first = lax.dynamic_slice_in_dim(array, core * (array.shape[0] // 2), array.shape[0] // 2)
    other = (1 - core) * (array.shape[0] // 2)
    return first, lax.dynamic_slice_in_dim(array, other, array.shape[0] // 2)


def end_kernel(row_ref, values_ref, gain_ref, out_ref):
    values = values_ref[...]
    inv = lax.rsqrt(jnp.mean(values * values, axis=1, keepdims=True) + norm_eps)
    scaled = jnp.sum(row_ref[...].astype(f32), axis=0) * gain_ref[...]
    mean = jnp.mean(values * scaled, axis=1, keepdims=True)
    out_ref[...] = inv * (scaled - values * inv * inv * mean)


def head_kernel(base_ref, normed_ref, own_ref, other_ref, bias_ref, goals_ref, stats_ref, scores_ref):
    half, ncols = normed_ref.shape[0], own_ref.shape[1]
    vocab = (own_ref, other_ref)
    normed, goals = normed_ref[...], goals_ref[...]
    scores = [dot(normed, v[...], 1, 0) + bias_ref[k : k + 1] for k, v in enumerate(vocab)]
    ids = lax.broadcasted_iota(jnp.int32, (half, ncols), 1)
    hit = [ids + base_ref[k] == goals for k in range(2)]
    top = jnp.maximum(*(jnp.max(s, axis=1, keepdims=True) for s in scores))
    total = sum(jnp.sum(jnp.exp(s - top), axis=1, keepdims=True) for s in scores)
    goal = sum(jnp.sum(jnp.where(h, s, 0.0), axis=1, keepdims=True) for h, s in zip(hit, scores))
    lane = lax.broadcasted_iota(jnp.int32, (half, half), 1)
    both = jnp.where(lane == 0, top + jnp.log(total), jnp.where(lane == 1, goal, 0.0)).T[:2]
    for k in range(stats_ref.shape[0]):
        stats_ref[k] = both
    for k in range(2):
        scores_ref[k] = scores[k]


def rows_kernel(base_ref, stats_ref, scores_ref, own_ref, other_ref, goals_ref, block_ref, dscore_ref, losses_ref):
    ncols = own_ref.shape[1]
    blocks, span, width = block_ref.shape
    half = blocks * span
    stats = stats_ref[...]
    tops = jnp.max(stats, axis=0)
    lse = tops + jnp.log(jnp.sum(jnp.exp(stats - tops), axis=0))
    lse, goal = lse[:1], jnp.sum(stats, axis=0)[1:]
    losses_ref[...] = lse - goal + zloss_weight * lse * lse
    lse = jnp.broadcast_to(lse, (half, half)).T[:, :1]
    scale = 1.0 + 2.0 * zloss_weight * lse
    ids = lax.broadcasted_iota(jnp.int32, (half, ncols), 1)
    dscore = []
    for k in range(2):
        hit = ids + base_ref[k] == goals_ref[...]
        d = jnp.exp(scores_ref[k] - lse) * scale - jnp.where(hit, 1.0, 0.0)
        dscore.append(d.astype(bf16))
        dscore_ref[:, k * ncols : (k + 1) * ncols] = dscore[k]
    for at in range(0, width, 512):
        terms = sum(dot(d, v[at : at + 512], 1, 1) for d, v in zip(dscore, (own_ref, other_ref))).astype(bf16)
        for k in range(blocks):
            block_ref[k, :, at : at + 512] = terms[k * span : (k + 1) * span]


def body(stream, hidden, w_down, final_gain, vocab, vocab_bias, targets):
    nz, nx, nc, ny = (lax.axis_size(a) for a in (Z, X, C, "dp"))
    z, x, c, y = (lax.axis_index(a) for a in (Z, X, C, "dp"))
    nq = nx * nc
    own, width = stream.shape
    group, units = hidden.shape
    cols = w_down.shape[1]
    ncols = vocab.shape[1]
    mine = (z * nx + x) * nc + c
    span = nz * own
    half = nx * span
    feats = nq * cols
    rows = -(-(units + own) // 16) * 16

    order = np.arange(group).reshape(nz, nq, own).transpose(1, 0, 2).reshape(-1)
    order = jnp.asarray(np.eye(group, dtype=np.float32)[order], bf16)
    mine_h = hidden.T
    part = stream.reshape(own, nz, feats).transpose(1, 0, 2)
    part = jnp.pad(part, ((0, 0), (units, rows - units - own), (0, group - feats)))
    mine_h = jnp.pad(mine_h, ((0, rows - units), (0, 0)))
    first = exchange(mine_h[None] + part, Z)

    blocks = w_down.T.reshape(cols, nz, nq, units).transpose(2, 0, 1, 3)
    blocks = jnp.pad(blocks, ((0, 0), (0, 0), (0, 0), (0, rows - units)))
    blocks = blocks.reshape(nx, nc, cols, nz * rows).transpose(1, 0, 2, 3)
    kept, sent = halves(blocks, c)
    came = partner(sent, C, 1)
    pair = jnp.concatenate([jnp.where(c == 0, kept, came), jnp.where(c == 0, came, kept)], axis=0)
    pair = pair.transpose(1, 0, 2, 3)
    w_rows = jnp.zeros_like(pair)
    for step in range(nx):
        block = lax.dynamic_slice_in_dim(pair, x ^ step, 1)
        block = partner(block, X, step) if step else block
        w_rows = lax.dynamic_update_slice_in_dim(w_rows, block, x ^ step, 0)

    sorted_h = dot(order, first.reshape(nz * rows, group), 1, 1).astype(bf16)
    partial = dot(sorted_h, w_rows.reshape(feats, nz * rows), 1, 1)
    proj = jnp.sum(exchange(partial.reshape(nq, span, feats), Q), axis=0)
    first, proj = lax.optimization_barrier((first, proj))
    row_part = first[:, units : units + own, :feats].reshape(span, feats)
    normin = (row_part.astype(f32) + proj).astype(bf16)
    gathered = shared(normin, Z, nz)
    values = gathered.transpose(1, 0, 2).reshape(span, width).astype(f32)
    inv = lax.rsqrt(jnp.mean(values * values, axis=1, keepdims=True) + norm_eps)
    normed = (values * inv * final_gain).astype(bf16)
    normed = shared(normed, X, nx).reshape(half, width)

    vocab = (vocab, partner(vocab, C, 1))
    bias = (vocab_bias, partner(vocab_bias.reshape(2, -1), C, 1).reshape(-1))

    line = lax.broadcasted_iota(jnp.int32, (half, group), 0)
    token = (line // own) % nz * (nq * own) + line // span * (nc * own) + c * own + line % own
    goals = jnp.where(token == lax.broadcasted_iota(jnp.int32, (half, group), 1), targets[None, :], 0)
    goals = jnp.sum(goals, axis=1)
    feat_group, last = width // ny, ny - 1
    early = lax.dynamic_slice_in_dim(normed, (y ^ last) * feat_group, feat_group, 1)
    early = partner(early, "dp", last)

    vmem, smem = (pl.BlockSpec(memory_space=m) for m in (pltpu.VMEM, pltpu.SMEM))
    base, goals = jnp.stack([mine * ncols, (mine ^ 1) * ncols]), goals[:, None]
    params = pltpu.CompilerParams(vmem_limit_bytes=24 << 20)
    cost = pl.CostEstimate(
        flops=4 * half * ncols * width, bytes_accessed=4 * ncols * width, transcendentals=2 * half * ncols
    )
    stats, scores = pl.pallas_call(
        head_kernel,
        out_shape=(
            jax.ShapeDtypeStruct((nx, 2, half), f32),
            jax.ShapeDtypeStruct((2, half, ncols), f32),
        ),
        in_specs=[smem] + [vmem] * 5,
        out_specs=(vmem,) * 2,
        compiler_params=params,
        cost_estimate=cost,
    )(base, normed, *vocab, jnp.stack(bias), goals)
    stats = merged(exchange(stats, X))
    stats = shared(stats, Z, nz)
    row_term, dscore, losses = pl.pallas_call(
        rows_kernel,
        out_shape=(
            jax.ShapeDtypeStruct((nx, span, width), bf16),
            jax.ShapeDtypeStruct((half, 2 * ncols), bf16),
            jax.ShapeDtypeStruct((1, half), f32),
        ),
        in_specs=[smem] + [vmem] * 5,
        out_specs=(vmem,) * 3,
        compiler_params=params,
        cost_estimate=cost,
    )(base, stats, scores, *vocab, goals)
    row_term, dscore, losses = lax.optimization_barrier((row_term, dscore, losses))
    losses = lax.dynamic_slice_in_dim(losses[0], x * span + z * own, own)

    row_x = exchange(row_term, X)
    row_x = jnp.sum(row_x.astype(f32), axis=0).astype(bf16)
    early, row_x = lax.optimization_barrier((early, row_x))
    early = jnp.where(c >= 0, early, 0)
    early = lax.optimization_barrier(early)
    theirs, ours = 0.0, 0.0
    for step in (0, 1, ny // 2, last):
        if step == last:
            piece, cols_of = early, partner(dscore, "dp", step)
        else:
            piece, cols_of = lax.dynamic_slice_in_dim(normed, (y ^ step) * feat_group, feat_group, 1), dscore
            if step:
                piece = partner(jnp.concatenate([piece, cols_of], axis=1), "dp", step)
                piece, cols_of = piece[:, :feat_group], piece[:, feat_group:]
        theirs = theirs + dot(piece, cols_of[:, ncols:], 0, 0)
        ours = ours + dot(piece, cols_of[:, :ncols], 0, 0)
    grad_vocab = lax.optimization_barrier(ours) + partner(theirs, C, 1)

    row_z = exchange(row_x.reshape(nz, own, width), Z)
    gathered, _ = lax.optimization_barrier((gathered, row_x))
    normin = lax.dynamic_slice_in_dim(gathered, z * own, own, 1).transpose(1, 0, 2).reshape(own, width)
    grad_input = pl.pallas_call(
        end_kernel,
        out_shape=jax.ShapeDtypeStruct((own, width), f32),
        in_specs=[pl.BlockSpec(memory_space=pltpu.VMEM)] * 3,
        out_specs=pl.BlockSpec(memory_space=pltpu.VMEM),
        compiler_params=pltpu.CompilerParams(vmem_limit_bytes=4 << 20),
    )(row_z, normin.astype(f32), final_gain[None])
    return (losses, grad_input, grad_vocab)


def solution(mesh):
    torus = Mesh(mesh.devices.reshape(16, 4, 2, mesh.shape["dp"]), ("vp_0", "vp_1", "vp_2", "dp"))
    return jax.shard_map(
        body,
        mesh=torus,
        in_specs=(P(DP_VP, None), P("dp", VP), P(None, VP), P(), P(None, VP), P(VP), P("dp")),
        out_specs=(P(DP_VP), P(DP_VP, None), P("dp", VP)),
        check_vma=False,
    )
```
